512 devices in a mesh: tp: 16 (over y, x), dp: 32 (over z, core).
Axes of the slice: x: 4, y: 4, z: 16, core: 2. Of those that a mesh axis runs over, the one named last changes fastest.
Arguments:
- stream: bfloat16 [64, 4096], P('tp', 'dp'), may hold values from -48 to 48
- norm_gain: float32 [2, 4096], P(None, 'dp'), may hold values from 0.1 to 1.9
- x_weight: bfloat16 [2, 4096, 8192], P(None, 'dp', 'tp'), may hold values from -0.09375 to 0.09375
- z_weight: bfloat16 [2, 4096, 8192], P(None, 'dp', 'tp'), may hold values from -0.09375 to 0.09375
- bc_weight: bfloat16 [2, 4096, 2, 2048], P(None, 'dp', None, 'tp'), may hold values from -0.09375 to 0.09375
- step_weight: bfloat16 [2, 4096, 128], P(None, 'dp'), may hold values from -0.09375 to 0.09375
- conv_x_weight: bfloat16 [2, 5, 8192], P(None, None, 'tp'), may hold values from -2.5 to 2.5
- conv_bc_weight: bfloat16 [2, 5, 2, 2048], P(None, None, None, 'tp'), may hold values from -2.5 to 2.5
- step_bias: float32 [2, 128], P(None, 'tp'), may hold values from -4 to 0.5
- decay_log: float32 [2, 128], P(None, 'tp'), may hold values from 0 to 2.8
- skip_gain: float32 [2, 128], P(None, 'tp'), may hold values from 0.1 to 1.9
- group_gain: float32 [2, 8192], P(None, 'tp'), may hold values from 0.1 to 1.9
- out_weight: bfloat16 [2, 8192, 4096], P(None, 'tp', 'dp'), may hold values from -0.0625 to 0.0625
- scan_state: float32 [2, 64, 128, 64, 128], P(None, 'dp', 'tp'), may hold values from -1.2 to 1.2
- conv_x_state: bfloat16 [2, 64, 4, 8192], P(None, 'dp', None, 'tp'), may hold values from -6 to 6
- conv_bc_state: bfloat16 [2, 64, 4, 2, 2048], P(None, 'dp', None, None, 'tp'), may hold values from -6 to 6
Outputs:
- stream_out: bfloat16 [64, 4096], P('tp', 'dp')
- scan_state_out: float32 [2, 64, 128, 64, 128], P(None, 'dp', 'tp')
- conv_x_out: bfloat16 [2, 64, 4, 8192], P(None, 'dp', None, 'tp')
- conv_bc_out: bfloat16 [2, 64, 4, 2, 2048], P(None, 'dp', None, None, 'tp')
The draws below stay inside these ranges and needn't reach their ends.
All inputs are finite; a program needn't handle non-finite values.
Results may differ from the reference program's by a relative error of at most 0.04.
Values may be sent and summed in bfloat16 or wider, within the bound.
No kernel may reach another device: no remote copies, remote signals or barrier semaphores. Data moves between devices by JAX's collectives and lax.ppermute only.
A program may use at most 64 MiB of HBM per device.

```python
import jax
import jax.numpy as jnp
from jax import lax

MODEL_WIDTH = 4096
HEAD_COUNT = 128
HEAD_DIM = 64
STATE_DIM = 128
GROUPS = 16
KERNEL = 5
LAYERS = 2
SEQUENCES = 64
INNER_WIDTH = 8192
BC_WIDTH = 2048
GROUP_WIDTH = 512
N_DP = 32


def draw_stream(key, part):
    base_key = jax.random.fold_in(key, 11)
    first, second, third = jax.random.split(base_key, 3)
    block_scale = jnp.exp(jax.random.uniform(second, (32,), jnp.float32, jnp.log(0.35), jnp.log(2.8)))
    column_scale = jnp.repeat(block_scale, MODEL_WIDTH // 32)
    values = jnp.clip(jax.random.normal(first, (SEQUENCES, MODEL_WIDTH), jnp.float32), -4.0, 4.0)
    return (values * column_scale[None, :]).astype(jnp.bfloat16)


def shard_levels(stream_key, shape, pieces, least, largest):
    level, own = 1.0, jax.random.fold_in(stream_key, 6)
    for position, shards_of in pieces:
        steps = jnp.exp(jax.random.uniform(jax.random.fold_in(own, position), (shards_of,), jnp.float32, least / len(pieces), largest / len(pieces)))
        level = level * jnp.repeat(steps, shape[position] // shards_of).reshape([-1 if axis == position else 1 for axis in range(len(shape))])
    return level


def gaussian(key, extent, width, bound, cuts=(), kind=jnp.bfloat16):
    entries = width * jax.random.normal(key, extent, jnp.float32)
    if cuts:
        entries = entries * shard_levels(key, extent, cuts, -0.22, 0.18)
    return jnp.clip(entries, -bound, bound).astype(kind)


def setup_inputs(seed: int = 0) -> dict:
    key_of = jax.random.split(jax.random.key(seed), 17)
    return {
        "stream": draw_stream(jax.random.fold_in(key_of[16], 71), 0),
        "norm_gain": jnp.clip(1.0 + 0.18 * jax.random.normal(key_of[1], (LAYERS, MODEL_WIDTH), jnp.float32), 0.1, 1.9),
        "x_weight": gaussian(key_of[2], (LAYERS, MODEL_WIDTH, INNER_WIDTH), MODEL_WIDTH ** -0.5, 0.09375, ((1, 32), (2, 16))),
        "z_weight": gaussian(key_of[3], (LAYERS, MODEL_WIDTH, INNER_WIDTH), MODEL_WIDTH ** -0.5, 0.09375, ((1, 32), (2, 16))),
        "bc_weight": gaussian(key_of[4], (LAYERS, MODEL_WIDTH, 2, BC_WIDTH), MODEL_WIDTH ** -0.5, 0.09375, ((1, 32), (3, 16))),
        "step_weight": gaussian(key_of[5], (LAYERS, MODEL_WIDTH, HEAD_COUNT), MODEL_WIDTH ** -0.5, 0.09375, ((1, 32),)),
        "conv_x_weight": gaussian(key_of[6], (LAYERS, KERNEL, INNER_WIDTH), KERNEL ** -0.5, 2.5, ((2, 16),)),
        "conv_bc_weight": gaussian(key_of[7], (LAYERS, KERNEL, 2, BC_WIDTH), KERNEL ** -0.5, 2.5, ((3, 16),)),
        "step_bias": jnp.clip(-4.0 + 4.5 * jax.random.uniform(key_of[8], (LAYERS, HEAD_COUNT), jnp.float32) ** shard_levels(key_of[8], (LAYERS, HEAD_COUNT), ((1, 16),), -0.2, 0.2), -4.0, 0.5),
        "decay_log": jnp.clip(2.8 * jax.random.uniform(key_of[9], (LAYERS, HEAD_COUNT), jnp.float32) ** shard_levels(key_of[9], (LAYERS, HEAD_COUNT), ((1, 16),), -0.2, 0.2), 0.0, 2.8),
        "skip_gain": jnp.clip(1.0 + 0.18 * jax.random.normal(key_of[10], (LAYERS, HEAD_COUNT), jnp.float32), 0.1, 1.9),
        "group_gain": jnp.clip(1.0 + 0.18 * jax.random.normal(key_of[11], (LAYERS, INNER_WIDTH), jnp.float32), 0.1, 1.9),
        "out_weight": gaussian(key_of[12], (LAYERS, INNER_WIDTH, MODEL_WIDTH), INNER_WIDTH ** -0.5, 0.0625, ((1, 16), (2, 32))),
        "scan_state": gaussian(key_of[13], (LAYERS, SEQUENCES, HEAD_COUNT, HEAD_DIM, STATE_DIM), 0.2, 1.2, ((1, 32), (2, 16)), jnp.float32),
        "conv_x_state": gaussian(key_of[14], (LAYERS, SEQUENCES, KERNEL - 1, INNER_WIDTH), 1.0, 6.0, ((1, 32), (3, 16))),
        "conv_bc_state": gaussian(key_of[15], (LAYERS, SEQUENCES, KERNEL - 1, 2, BC_WIDTH), 1.0, 6.0, ((1, 32), (4, 16))),
    }


EPS = 1e-06

def block_rounded(values):
    rounded = lax.optimization_barrier(values.astype(jnp.bfloat16))
    return lax.optimization_barrier(jnp.sum(rounded.astype(jnp.float32), axis=1))

def split_product(normed_in, weight):
    row_count = normed_in.shape[0]
    columns = weight.shape[1]
    block_rows = MODEL_WIDTH // N_DP
    left = normed_in.astype(jnp.float32).reshape(row_count, N_DP, block_rows)
    right = weight.astype(jnp.float32).reshape(N_DP, block_rows, columns)
    partials = jnp.einsum('skw,kwc->skc', left, right)
    return block_rounded(partials)

def mixer_block(stream, norm_gain, x_weight, z_weight, bc_weight, step_weight, conv_x_weight, conv_bc_weight, step_bias, decay_log, skip_gain, group_gain, out_weight, scan_state, conv_x_state, conv_bc_state):
    row_count = stream.shape[0]
    per_group = HEAD_COUNT // GROUPS
    widened = stream.astype(jnp.float32)
    normed_in = (widened * norm_gain).astype(jnp.bfloat16)
    square_part = lax.optimization_barrier(jnp.sum((widened * widened).reshape(row_count, N_DP, MODEL_WIDTH // N_DP), axis=2))
    inv_rms = lax.rsqrt(block_rounded(square_part)[:, None] / MODEL_WIDTH + EPS)
    proj_x = (split_product(normed_in, x_weight) * inv_rms).astype(jnp.bfloat16)
    proj_z = (split_product(normed_in, z_weight) * inv_rms).astype(jnp.bfloat16)
    proj_bc = (split_product(normed_in, bc_weight.reshape(MODEL_WIDTH, 2 * BC_WIDTH)) * inv_rms).astype(jnp.bfloat16)
    proj_bc = proj_bc.reshape(row_count, 2, BC_WIDTH)
    step_raw = split_product(normed_in, step_weight) * inv_rms
    window_x = jnp.concatenate([conv_x_state, proj_x[:, None, :]], axis=1)
    inputs_x = jax.nn.silu(lax.optimization_barrier(jnp.sum(window_x.astype(jnp.float32) * conv_x_weight.astype(jnp.float32), axis=1)))
    window_bc = jnp.concatenate([conv_bc_state, proj_bc[:, None]], axis=1)
    inputs_bc = jax.nn.silu(lax.optimization_barrier(jnp.sum(window_bc.astype(jnp.float32) * conv_bc_weight.astype(jnp.float32), axis=1)))
    b_part = inputs_bc[:, 0].reshape(row_count, GROUPS, STATE_DIM)
    c_part = inputs_bc[:, 1].reshape(row_count, GROUPS, STATE_DIM)
    step_size = jax.nn.softplus(step_raw + step_bias)
    decay_rate = jnp.exp(-step_size * jnp.exp(decay_log))
    heads_x = inputs_x.reshape(row_count, GROUPS, per_group, HEAD_DIM)
    step_heads = step_size.reshape(row_count, GROUPS, per_group)
    decay_heads = decay_rate.reshape(row_count, GROUPS, per_group)
    old_state = scan_state.reshape(row_count, GROUPS, per_group, HEAD_DIM, STATE_DIM)
    state_new = old_state * decay_heads[..., None, None] + (step_heads[..., None] * heads_x)[..., None] * b_part[:, :, None, None, :]
    readout = jnp.einsum('sgepn,sgn->sgep', state_new, c_part, precision=lax.Precision.HIGHEST)
    readout = readout + skip_gain.reshape(GROUPS, per_group)[None, :, :, None] * heads_x
    gated_out = readout.reshape(row_count, INNER_WIDTH) * jax.nn.silu(proj_z.astype(jnp.float32))
    grouped = gated_out.reshape(row_count, GROUPS, GROUP_WIDTH)
    normed = grouped * lax.rsqrt(lax.optimization_barrier(jnp.mean(grouped * grouped, axis=2, keepdims=True)) + EPS)
    mixed_rows = (normed.reshape(row_count, INNER_WIDTH) * group_gain).astype(jnp.bfloat16)
    update = jnp.dot(mixed_rows, out_weight, preferred_element_type=jnp.float32)
    stream_next = (widened + update).astype(jnp.bfloat16)
    return (stream_next, state_new.reshape(row_count, HEAD_COUNT, HEAD_DIM, STATE_DIM), window_x[:, 1:], window_bc[:, 1:])

def reference(stream, norm_gain, x_weight, z_weight, bc_weight, step_weight, conv_x_weight, conv_bc_weight, step_bias, decay_log, skip_gain, group_gain, out_weight, scan_state, conv_x_state, conv_bc_state):
    current = stream
    states_list = []
    xconv_list = []
    bcconv_list = []
    for block_index in range(LAYERS):
        current, state_next, xconv_next, bcconv_next = mixer_block(current, norm_gain[block_index], x_weight[block_index], z_weight[block_index], bc_weight[block_index], step_weight[block_index], conv_x_weight[block_index], conv_bc_weight[block_index], step_bias[block_index], decay_log[block_index], skip_gain[block_index], group_gain[block_index], out_weight[block_index], scan_state[block_index], conv_x_state[block_index], conv_bc_state[block_index])
        states_list.append(state_next)
        xconv_list.append(xconv_next)
        bcconv_list.append(bcconv_next)
    return (current, jnp.stack(states_list), jnp.stack(xconv_list), jnp.stack(bcconv_list))
```

```python
import jax
import jax.numpy as jnp
from jax import lax
from jax.sharding import Mesh, PartitionSpec as P

MODEL_WIDTH = 4096
HEAD_COUNT = 128
HEAD_DIM = 64
STATE_DIM = 128
LAYERS = 2
EPS = 1e-06

TP = ("y", "x")
CTP = ("core", "y", "x")


def exchange(value, axis):
    return lax.all_to_all(value, axis, split_axis=0, concat_axis=0, tiled=True)


def to_all(value, count):
    return jnp.broadcast_to(value, (count, *value.shape))


def shards(
    stream,
    norm_gain,
    x_weight,
    z_weight,
    bc_weight,
    step_weight,
    conv_x_weight,
    conv_bc_weight,
    step_bias,
    decay_log,
    skip_gain,
    group_gain,
    out_weight,
    scan_state,
    conv_x_state,
    conv_bc_state,
):
    f32, bf16 = jnp.float32, jnp.bfloat16
    n_tp, n_z = lax.axis_size(TP), lax.axis_size("z")
    tp_index = lax.axis_index(TP)
    rows_dev = stream.shape[0]
    cols_dev = stream.shape[1]
    seq_count = scan_state.shape[1]
    heads_dev = scan_state.shape[2]
    x_width = x_weight.shape[2]
    bc_width = 2 * bc_weight.shape[3]
    groups_dev = conv_bc_state.shape[4] // STATE_DIM
    per_group = heads_dev // groups_dev
    seqs = n_z * seq_count

    def in_weights(l):
        step_cols = lax.dynamic_slice_in_dim(step_weight[l], tp_index * heads_dev, heads_dev, 1)
        return jnp.concatenate(
            [x_weight[l], z_weight[l], bc_weight[l].reshape(cols_dev, bc_width), step_cols], axis=1
        )

    own = jnp.broadcast_to(
        stream.reshape(2, 1, rows_dev // 2, cols_dev), (2, n_tp, rows_dev // 2, cols_dev)
    )
    hidden = exchange(own.reshape(2 * n_tp, rows_dev // 2, cols_dev), CTP).reshape(2, seqs, cols_dev)
    w_in = [exchange(to_all(in_weights(l), 2), "core") for l in range(LAYERS)]
    w_out = exchange(to_all(out_weight, 2), "core")
    gain = exchange(to_all(norm_gain, 2), "core")

    states_list, xconv_list, bcconv_list = [], [], []
    result = None
    for l in range(LAYERS):
        widened = hidden.astype(f32)
        normed_in = (widened * gain[:, l][:, None, :]).astype(bf16)
        part_sq = jnp.sum(widened * widened, axis=(0, 2))[:, None]
        part = sum(
            jnp.dot(normed_in[c], w_in[l][c], preferred_element_type=f32) for c in range(2)
        )
        part = jnp.concatenate([part, part_sq], axis=1).astype(bf16)
        got = exchange(part.reshape(n_z, seq_count, -1), "z").astype(f32).sum(axis=0)
        inv_rms = lax.rsqrt(got[:, -1:] / MODEL_WIDTH + EPS)
        proj = got * inv_rms
        proj_x = proj[:, :x_width].astype(bf16)
        proj_z = proj[:, x_width : 2 * x_width].astype(bf16)
        proj_bc = proj[:, 2 * x_width : 2 * x_width + bc_width].astype(bf16)
        proj_bc = proj_bc.reshape(seq_count, 2, -1)
        step_raw = proj[:, 2 * x_width + bc_width : -1]
        window_x = jnp.concatenate([conv_x_state[l], proj_x[:, None, :]], axis=1)
        inputs_x = jax.nn.silu(
            jnp.sum(window_x.astype(f32) * conv_x_weight[l].astype(f32), axis=1)
        )
        window_bc = jnp.concatenate([conv_bc_state[l], proj_bc[:, None]], axis=1)
        inputs_bc = jax.nn.silu(
            jnp.sum(window_bc.astype(f32) * conv_bc_weight[l].astype(f32), axis=1)
        )
        b_part = inputs_bc[:, 0].reshape(seq_count, groups_dev, STATE_DIM)
        c_part = inputs_bc[:, 1].reshape(seq_count, groups_dev, STATE_DIM)
        step_size = jax.nn.softplus(step_raw + step_bias[l])
        decay_rate = jnp.exp(-step_size * jnp.exp(decay_log[l]))
        heads_x = inputs_x.reshape(seq_count, groups_dev, per_group, HEAD_DIM)
        step_heads = step_size.reshape(seq_count, groups_dev, per_group)
        decay_heads = decay_rate.reshape(seq_count, groups_dev, per_group)
        old_state = scan_state[l].reshape(seq_count, groups_dev, per_group, HEAD_DIM, STATE_DIM)
        state_new = (
            old_state * decay_heads[..., None, None]
            + (step_heads[..., None] * heads_x)[..., None] * b_part[:, :, None, None, :]
        )
        readout = jnp.einsum("sgepn,sgn->sgep", state_new, c_part)
        readout = (
            readout + skip_gain[l].reshape(groups_dev, per_group)[None, :, :, None] * heads_x
        )
        gated_out = readout.reshape(seq_count, -1) * jax.nn.silu(proj_z.astype(f32))
        grouped = gated_out.reshape(seq_count, groups_dev, -1)
        normed = grouped * lax.rsqrt(jnp.mean(grouped * grouped, axis=2, keepdims=True) + EPS)
        mixed_rows = (normed.reshape(seq_count, -1) * group_gain[l]).astype(bf16)
        states_list.append(state_new.reshape(seq_count, heads_dev, HEAD_DIM, STATE_DIM))
        xconv_list.append(window_x[:, 1:])
        bcconv_list.append(window_bc[:, 1:])

        mixed = exchange(to_all(mixed_rows, n_z), "z").reshape(seqs, -1)
        terms = jnp.stack(
            [jnp.dot(mixed, w_out[c, l], preferred_element_type=f32) for c in range(2)]
        ).astype(bf16)
        if l + 1 < LAYERS:
            summed = exchange(to_all(terms, n_tp), TP).astype(f32).sum(axis=0)
            hidden = (widened + summed).astype(bf16)
        else:
            both = jnp.concatenate(
                [
                    terms.reshape(2 * n_tp, rows_dev // 2, cols_dev),
                    hidden.reshape(2 * n_tp, rows_dev // 2, cols_dev),
                ],
                axis=1,
            )
            arrived = exchange(both, CTP).reshape(2, n_tp, rows_dev, cols_dev).astype(f32)
            result = arrived[:, :, : rows_dev // 2].sum(axis=1) + arrived[:, 0, rows_dev // 2 :]
            result = result.astype(bf16).reshape(rows_dev, cols_dev)
    return (result, jnp.stack(states_list), jnp.stack(xconv_list), jnp.stack(bcconv_list))


def solution(mesh):
    fine = Mesh(mesh.devices.reshape(4, 4, -1, 2), ("y", "x", "z", "core"))
    dp = ("z", "core")
    in_specs = (
        P(TP, dp),
        P(None, dp),
        P(None, dp, TP),
        P(None, dp, TP),
        P(None, dp, None, TP),
        P(None, dp, None),
        P(None, None, TP),
        P(None, None, None, TP),
        P(None, TP),
        P(None, TP),
        P(None, TP),
        P(None, TP),
        P(None, TP, dp),
        P(None, dp, TP, None, None),
        P(None, dp, None, TP),
        P(None, dp, None, None, TP),
    )
    out_specs = (
        P(TP, dp),
        P(None, dp, TP, None, None),
        P(None, dp, None, TP),
        P(None, dp, None, None, TP),
    )
    return jax.shard_map(shards, mesh=fine, in_specs=in_specs, out_specs=out_specs, check_vma=False)
```

```python
import functools

import jax
import jax.numpy as jnp
from jax import lax
from jax.experimental import pallas as pl
from jax.experimental.pallas import tpu as pltpu
from jax.sharding import Mesh, PartitionSpec as P


MODEL_WIDTH = 4096
HEAD_DIM = 64
STATE_DIM = 128
LAYERS = 2
EPS = 1e-06
LANES = 128

TP = ("y", "x")
CTP = ("core", "y", "x")
VMEM = pl.BlockSpec(memory_space=pltpu.VMEM)
SMEM = pl.BlockSpec(memory_space=pltpu.SMEM)
f32, bf16 = jnp.float32, jnp.bfloat16


def exchange(value, axis):
    return lax.all_to_all(value, axis, split_axis=0, concat_axis=0, tiled=True)


def swap_cores(value):
    return lax.ppermute(value, "core", [(0, 1), (1, 0)])


def to_all(value, count):
    return jnp.broadcast_to(value, (count, *value.shape))


def call(body, out_shape, n_in, flops, size, smem=0):
    return pl.pallas_call(
        body,
        out_shape=out_shape,
        in_specs=[SMEM] * smem + [VMEM] * (n_in - smem),
        out_specs=jax.tree.map(lambda _: VMEM, out_shape),
        compiler_params=pltpu.CompilerParams(vmem_limit_bytes=8 * 1024 * 1024),
        cost_estimate=pl.CostEstimate(flops=flops, bytes_accessed=size, transcendentals=0),
    )


def put_projections(layer, x_ref, z_ref, bc_ref, step_ref, out_ref):
    at = 0
    for ref in (x_ref, z_ref, bc_ref, step_ref):
        for k in range(ref.shape[2] // LANES):
            out_ref[at] = ref[layer, :, k * LANES : (k + 1) * LANES]
            at += 1
    return at


def pack_first(x_ref, z_ref, bc_ref, step_ref, out_ref):
    put_projections(0, x_ref, z_ref, bc_ref, step_ref, out_ref)


def pack_rest(x_ref, z_ref, bc_ref, step_ref, w_ref, gain_ref, out_ref):
    at = put_projections(1, x_ref, z_ref, bc_ref, step_ref, out_ref)
    for l in range(LAYERS):
        for k in range(w_ref.shape[1] // LANES):
            out_ref[at] = w_ref[l, k * LANES : (k + 1) * LANES, :]
            at += 1
    gain = gain_ref[1:2, :]
    first = gain.astype(bf16)
    left = gain - first.astype(f32)
    second = left.astype(bf16)
    third = (left - second.astype(f32)).astype(bf16)
    row = lax.broadcasted_iota(jnp.int32, (LANES, LANES), 0)
    pieces = jnp.where(
        row == 0,
        first.astype(f32),
        jnp.where(row == 1, second.astype(f32), jnp.where(row == 2, third.astype(f32), 0.0)),
    ).astype(bf16)
    out_ref[at] = pieces


def project(normed, squares, first, weights, place, out_ref, blocks):
    total = None
    for rows, w_ref in zip(normed, weights):
        block = jnp.concatenate([w_ref[k] for k in range(blocks)], axis=1)
        term = jnp.dot(rows, block, preferred_element_type=f32)
        total = term if total is None else total + term
    wide = (blocks - 1) * LANES
    out_ref[:, :wide] = total[:, :wide].astype(bf16)
    lane = lax.broadcasted_iota(jnp.int32, (total.shape[0], LANES), 1)
    tail = pltpu.roll(total[:, wide:], LANES - place, 1)
    tail = jnp.where(lane == first, squares, tail)
    out_ref[:, wide:] = tail.astype(bf16)


def project_first(blocks, heads, place_ref, hidden_ref, normed_ref, own_ref, other_ref, out_ref):
    core = place_ref[1]
    wide = [hidden_ref[c].astype(f32) for c in range(2)]
    squares = jnp.sum(wide[0] * wide[0] + wide[1] * wide[1], axis=1, keepdims=True)
    normed = [normed_ref[core], normed_ref[1 - core]]
    project(normed, squares, heads, (own_ref, other_ref), place_ref[0], out_ref, blocks)


def project_next(
    blocks, heads, place_ref, arrived_ref, hidden_ref, own_ref, other_ref, out_ref, next_ref
):
    core = place_ref[1]
    wide, normed = [], []
    last = own_ref.shape[0] - 1
    for c, w_ref in ((core, own_ref), (1 - core, other_ref)):
        summed = arrived_ref[0, c].astype(f32)
        for j in range(1, arrived_ref.shape[0]):
            summed = summed + arrived_ref[j, c].astype(f32)
        new = (hidden_ref[c].astype(f32) + summed).astype(bf16)
        next_ref[c] = new
        pieces = w_ref[last].astype(f32)
        gain = pieces[0:1] + pieces[1:2] + pieces[2:3]
        wide.append(new.astype(f32))
        normed.append((new.astype(f32) * gain).astype(bf16))
    squares = jnp.sum(wide[0] * wide[0] + wide[1] * wide[1], axis=1, keepdims=True)
    project(normed, squares, heads, (own_ref, other_ref), place_ref[0], out_ref, blocks)


def out_terms(mixed_ref, w_ref, at, blocks):
    weights = jnp.concatenate([w_ref[at + k] for k in range(blocks)], axis=0)
    return jnp.dot(mixed_ref[...], weights, preferred_element_type=f32).astype(bf16)


def mix_to_all(at, blocks, place_ref, mixed_ref, own_ref, other_ref, out_ref):
    core = place_ref[1]
    for c, w_ref in ((core, own_ref), (1 - core, other_ref)):
        terms = out_terms(mixed_ref, w_ref, at, blocks)
        for j in range(out_ref.shape[0]):
            out_ref[j, c] = terms


def mix_last(at, blocks, place_ref, mixed_ref, own_ref, other_ref, out_ref):
    core = place_ref[1]
    for c, w_ref in ((core, own_ref), (1 - core, other_ref)):
        out_ref[c] = out_terms(mixed_ref, w_ref, at, blocks)


def shards(
    stream,
    norm_gain,
    x_weight,
    z_weight,
    bc_weight,
    step_weight,
    conv_x_weight,
    conv_bc_weight,
    step_bias,
    decay_log,
    skip_gain,
    group_gain,
    out_weight,
    scan_state,
    conv_x_state,
    conv_bc_state,
):
    n_tp, n_z = lax.axis_size(TP), lax.axis_size("z")
    tp_index = lax.axis_index(TP)
    rows_dev, cols_dev = stream.shape
    half = rows_dev // 2
    seq_count, heads_dev = scan_state.shape[1:3]
    x_width = x_weight.shape[2]
    bc_width = 2 * bc_weight.shape[3]
    groups_dev = conv_bc_state.shape[4] // STATE_DIM
    per_group = heads_dev // groups_dev
    seqs = n_z * seq_count
    in_blocks = (2 * x_width + bc_width) // LANES + 1
    out_blocks = x_width // LANES
    rest = in_blocks + LAYERS * out_blocks + 1
    wide = in_blocks * LANES
    place = jnp.stack([tp_index * heads_dev, lax.axis_index("core")]).astype(jnp.int32)
    shape = jax.ShapeDtypeStruct

    normed_own = (stream.astype(f32) * norm_gain[0]).astype(bf16)
    own = jnp.stack([stream.reshape(2, half, cols_dev), normed_own.reshape(2, half, cols_dev)], 1)
    own = own.reshape(2, 1, rows_dev, cols_dev)
    own = jnp.broadcast_to(own, (2, n_tp, rows_dev, cols_dev))
    rows = exchange(own.reshape(2 * n_tp, rows_dev, cols_dev), CTP)
    bc_flat = bc_weight.reshape(LAYERS, cols_dev, bc_width)
    packed = call(
        pack_first, shape((in_blocks, cols_dev, LANES), bf16), 4, 1000000, 1000000
    )(x_weight, z_weight, bc_flat, step_weight)
    w_first = (packed, swap_cores(packed))
    packed = call(
        pack_rest, shape((rest, cols_dev, LANES), bf16), 6, 1000000, 1000000
    )(x_weight, z_weight, bc_flat, step_weight, out_weight, norm_gain)
    w_rest = (packed, swap_cores(packed))
    x_tap = conv_x_weight.astype(f32)
    bc_tap = conv_bc_weight.astype(f32)
    x_base = jnp.sum(conv_x_state.astype(f32) * x_tap[:, None, :-1], axis=2)
    bc_base = jnp.sum(conv_bc_state.astype(f32) * bc_tap[:, None, :-1], axis=2)
    rate = jnp.exp(decay_log)

    states_list, xconv_list, bcconv_list = [], [], []
    result = None
    hidden = None
    for l in range(LAYERS):
        if l == 0:
            rows = rows.reshape(2, n_tp, 2, half, cols_dev)
            hidden = rows[:, :, 0].reshape(2, seqs, cols_dev)
            normed_in = rows[:, :, 1].reshape(2, seqs, cols_dev)
            part = call(
                functools.partial(project_first, in_blocks, heads_dev),
                shape((seqs, wide), bf16), 5, 10000000, 1000000, smem=1,
            )(place, hidden, normed_in, *w_first)
        else:
            part, hidden = call(
                functools.partial(project_next, in_blocks, heads_dev),
                (shape((seqs, wide), bf16), shape((2, seqs, cols_dev), bf16)), 5, 10000000, 1000000, smem=1,
            )(place, arrived, hidden, *w_rest)
        got = exchange(part.reshape(n_z, seq_count, wide), "z")
        got = got.astype(f32).sum(axis=0)
        tail = wide - LANES
        inv_rms = lax.rsqrt(got[:, tail + heads_dev : tail + heads_dev + 1] / MODEL_WIDTH + EPS)
        proj_x = (got[:, :x_width] * inv_rms).astype(bf16)
        proj_z = (got[:, x_width : 2 * x_width] * inv_rms).astype(bf16)
        proj_bc = (got[:, 2 * x_width : tail] * inv_rms).astype(bf16).reshape(seq_count, 2, -1)
        step_raw = got[:, tail : tail + heads_dev] * inv_rms
        inputs_x = jax.nn.silu(x_base[l] + proj_x.astype(f32) * x_tap[l, -1])
        inputs_bc = jax.nn.silu(bc_base[l] + proj_bc.astype(f32) * bc_tap[l, -1])
        b_part = inputs_bc[:, 0].reshape(seq_count, groups_dev, STATE_DIM)
        c_part = inputs_bc[:, 1].reshape(seq_count, groups_dev, STATE_DIM)
        step_size = jax.nn.softplus(step_raw + step_bias[l])
        decay_rate = jnp.exp(-step_size * rate[l])
        heads_x = inputs_x.reshape(seq_count, groups_dev, per_group, HEAD_DIM)
        step_heads = step_size.reshape(seq_count, groups_dev, per_group)
        decay_heads = decay_rate.reshape(seq_count, groups_dev, per_group)
        old_state = scan_state[l].reshape(seq_count, groups_dev, per_group, HEAD_DIM, STATE_DIM)
        state_new = (
            old_state * decay_heads[..., None, None]
            + (step_heads[..., None] * heads_x)[..., None] * b_part[:, :, None, None, :]
        )
        readout = jnp.einsum("sgepn,sgn->sgep", state_new, c_part)
        readout = (
            readout + skip_gain[l].reshape(groups_dev, per_group)[None, :, :, None] * heads_x
        )
        gated_out = readout.reshape(seq_count, -1) * jax.nn.silu(proj_z.astype(f32))
        grouped = gated_out.reshape(seq_count, groups_dev, -1)
        normed = grouped * lax.rsqrt(jnp.mean(grouped * grouped, axis=2, keepdims=True) + EPS)
        mixed_rows = (normed.reshape(seq_count, -1) * group_gain[l]).astype(bf16)
        states_list.append(state_new.reshape(seq_count, heads_dev, HEAD_DIM, STATE_DIM))
        xconv_list.append(jnp.concatenate([conv_x_state[l, :, 1:], proj_x[:, None]], axis=1))
        bcconv_list.append(jnp.concatenate([conv_bc_state[l, :, 1:], proj_bc[:, None]], axis=1))

        mixed = exchange(to_all(mixed_rows, n_z), "z").reshape(seqs, -1)
        at = in_blocks + l * out_blocks
        if l + 1 < LAYERS:
            terms = call(
                functools.partial(mix_to_all, at, out_blocks),
                shape((n_tp, 2, seqs, cols_dev), bf16), 4, 10000000, 1000000, smem=1,
            )(place, mixed, *w_rest)
            arrived = exchange(terms, TP)
        else:
            terms = call(
                functools.partial(mix_last, at, out_blocks),
                shape((2, seqs, cols_dev), bf16), 4, 10000000, 1000000, smem=1,
            )(place, mixed, *w_rest)
            both = jnp.concatenate(
                [terms.reshape(2 * n_tp, half, cols_dev), hidden.reshape(2 * n_tp, half, cols_dev)],
                axis=1,
            )
            got = exchange(both, CTP).reshape(2, n_tp, rows_dev, cols_dev).astype(f32)
            result = got[:, :, :half].sum(axis=1) + got[:, 0, half:]
            result = result.astype(bf16).reshape(rows_dev, cols_dev)
    outs = (jnp.stack(states_list), jnp.stack(xconv_list), jnp.stack(bcconv_list))
    return (result, *outs)


def solution(mesh):
    fine = Mesh(mesh.devices.reshape(4, 4, -1, 2), ("y", "x", "z", "core"))
    dp = ("z", "core")
    in_specs = (
        P(TP, dp),
        P(None, dp),
        P(None, dp, TP),
        P(None, dp, TP),
        P(None, dp, None, TP),
        P(None, dp, None),
        P(None, None, TP),
        P(None, None, None, TP),
        P(None, TP),
        P(None, TP),
        P(None, TP),
        P(None, TP),
        P(None, TP, dp),
        P(None, dp, TP, None, None),
        P(None, dp, None, TP),
        P(None, dp, None, None, TP),
    )
    out_specs = (
        P(TP, dp),
        P(None, dp, TP, None, None),
        P(None, dp, None, TP),
        P(None, dp, None, None, TP),
    )
    return jax.shard_map(shards, mesh=fine, in_specs=in_specs, out_specs=out_specs, check_vma=False)
```

```python
import functools

import jax
import jax.numpy as jnp
from jax import lax
from jax.experimental import pallas as pl
from jax.experimental.pallas import tpu as pltpu
from jax.sharding import Mesh, PartitionSpec as P


MODEL_WIDTH = 4096
HEAD_DIM = 64
STATE_DIM = 128
LAYERS = 2
EPS = 1e-06
LANES = 128

TP = ("y", "x")
CTP = ("core", "y", "x")
VMEM = pl.BlockSpec(memory_space=pltpu.VMEM)
SMEM = pl.BlockSpec(memory_space=pltpu.SMEM)
f32, bf16 = jnp.float32, jnp.bfloat16


def exchange(value, axis):
    return lax.all_to_all(value, axis, split_axis=0, concat_axis=0, tiled=True)


def exchange_from_middle(value, count):
    order = [(count // 2 + k) % count for k in range(count)]
    return lax.all_to_all(
        value, "z", split_axis=0, concat_axis=0, axis_index_groups=[order], tiled=True
    )


def swap_cores(value):
    return lax.ppermute(value, "core", [(0, 1), (1, 0)])


def to_all(value, count):
    return jnp.broadcast_to(value, (count, *value.shape))


def call(body, out_shape, n_in, flops, size, smem=0):
    return pl.pallas_call(
        body,
        out_shape=out_shape,
        in_specs=[SMEM] * smem + [VMEM] * (n_in - smem),
        out_specs=jax.tree.map(lambda _: VMEM, out_shape),
        compiler_params=pltpu.CompilerParams(vmem_limit_bytes=8 * 1024 * 1024),
        cost_estimate=pl.CostEstimate(flops=flops, bytes_accessed=size, transcendentals=0),
    )


def put_projections(layer, x_ref, z_ref, bc_ref, step_ref, out_ref):
    at = 0
    for ref in (x_ref, z_ref, bc_ref, step_ref):
        for k in range(ref.shape[2] // LANES):
            out_ref[at] = ref[layer, :, k * LANES : (k + 1) * LANES]
            at += 1
    return at


def put_gain(gain, out_ref, at):
    first = gain.astype(bf16)
    left = gain - first.astype(f32)
    second = left.astype(bf16)
    third = (left - second.astype(f32)).astype(bf16)
    row = lax.broadcasted_iota(jnp.int32, (LANES, LANES), 0)
    pieces = jnp.where(row == 1, second.astype(f32), jnp.where(row == 2, third.astype(f32), 0.0))
    out_ref[at] = jnp.where(row == 0, first.astype(f32), pieces).astype(bf16)


def pack_first(x_ref, z_ref, bc_ref, step_ref, gain_ref, out_ref):
    at = put_projections(0, x_ref, z_ref, bc_ref, step_ref, out_ref)
    put_gain(gain_ref[0:1, :], out_ref, at)


def pack_rest(x_ref, z_ref, bc_ref, step_ref, w_ref, gain_ref, out_ref):
    at = put_projections(1, x_ref, z_ref, bc_ref, step_ref, out_ref)
    put_gain(gain_ref[1:2, :], out_ref, at)
    at += 1
    for l in range(LAYERS):
        for k in range(w_ref.shape[1] // LANES):
            out_ref[at] = w_ref[l, k * LANES : (k + 1) * LANES, :]
            at += 1


def project(normed, squares, first, weights, place, out_ref, blocks):
    total = None
    for rows, w_ref in zip(normed, weights):
        block = jnp.concatenate([w_ref[k] for k in range(blocks)], axis=1)
        term = jnp.dot(rows, block, preferred_element_type=f32)
        total = term if total is None else total + term
    wide = (blocks - 1) * LANES
    half = total.shape[0] // 2
    lane = lax.broadcasted_iota(jnp.int32, (total.shape[0], LANES), 1)
    tail = pltpu.roll(total[:, wide:], LANES - place, 1)
    tail = jnp.where(lane == first, squares, tail)
    for to, rows in ((0, slice(half, None)), (half, slice(0, half))):
        out_ref[to : to + half, :wide] = total[rows, :wide].astype(bf16)
        out_ref[to : to + half, wide:] = tail[rows].astype(bf16)


def scaled(rows, w_ref, blocks):
    pieces = w_ref[blocks, :8].astype(f32)
    gain = pieces[0:1] + pieces[1:2] + pieces[2:3]
    return (rows.astype(f32) * gain).astype(bf16)


def project_first(blocks, heads, place_ref, hidden_ref, own_ref, other_ref, out_ref):
    core = place_ref[1]
    rows = [hidden_ref[core], hidden_ref[1 - core]]
    wide = [r.astype(f32) for r in rows]
    squares = jnp.sum(wide[0] * wide[0] + wide[1] * wide[1], axis=1, keepdims=True)
    weights = (own_ref, other_ref)
    normed = [scaled(r, w, blocks) for r, w in zip(rows, weights)]
    project(normed, squares, heads, weights, place_ref[0], out_ref, blocks)


def project_next(
    blocks, heads, place_ref, arrived_ref, hidden_ref, own_ref, other_ref, out_ref, next_ref
):
    core = place_ref[1]
    rows = []
    weights = (own_ref, other_ref)
    for c in (core, 1 - core):
        summed = arrived_ref[0, c].astype(f32)
        for j in range(1, arrived_ref.shape[0]):
            summed = summed + arrived_ref[j, c].astype(f32)
        new = (hidden_ref[c].astype(f32) + summed).astype(bf16)
        next_ref[c] = new
        rows.append(new)
    wide = [r.astype(f32) for r in rows]
    squares = jnp.sum(wide[0] * wide[0] + wide[1] * wide[1], axis=1, keepdims=True)
    normed = [scaled(r, w, blocks) for r, w in zip(rows, weights)]
    project(normed, squares, heads, weights, place_ref[0], out_ref, blocks)


def out_terms(mixed_ref, w_ref, at, blocks):
    weights = jnp.concatenate([w_ref[at + k] for k in range(blocks)], axis=0)
    half = mixed_ref.shape[0] // 2
    mixed = jnp.concatenate([mixed_ref[half:], mixed_ref[:half]], axis=0)
    return jnp.dot(mixed, weights, preferred_element_type=f32).astype(bf16)


def mix_to_all(at, blocks, place_ref, mixed_ref, own_ref, other_ref, out_ref):
    core = place_ref[1]
    for c, w_ref in ((core, own_ref), (1 - core, other_ref)):
        terms = out_terms(mixed_ref, w_ref, at, blocks)
        for j in range(out_ref.shape[0]):
            out_ref[j, c] = terms


def mix_last(at, blocks, place_ref, mixed_ref, own_ref, other_ref, out_ref):
    core = place_ref[1]
    for c, w_ref in ((core, own_ref), (1 - core, other_ref)):
        out_ref[c] = out_terms(mixed_ref, w_ref, at, blocks)


def shards(
    stream,
    norm_gain,
    x_weight,
    z_weight,
    bc_weight,
    step_weight,
    conv_x_weight,
    conv_bc_weight,
    step_bias,
    decay_log,
    skip_gain,
    group_gain,
    out_weight,
    scan_state,
    conv_x_state,
    conv_bc_state,
):
    n_tp, n_z = lax.axis_size(TP), lax.axis_size("z")
    tp_index = lax.axis_index(TP)
    rows_dev, cols_dev = stream.shape
    half = rows_dev // 2
    seq_count, heads_dev = scan_state.shape[1:3]
    x_width = x_weight.shape[2]
    bc_width = 2 * bc_weight.shape[3]
    groups_dev = conv_bc_state.shape[4] // STATE_DIM
    per_group = heads_dev // groups_dev
    seqs = n_z * seq_count
    in_blocks = (2 * x_width + bc_width) // LANES + 1
    out_blocks = x_width // LANES
    rest = in_blocks + LAYERS * out_blocks + 1
    wide = in_blocks * LANES
    place = jnp.stack([tp_index * heads_dev, lax.axis_index("core")]).astype(jnp.int32)
    shape = jax.ShapeDtypeStruct

    own = jnp.broadcast_to(
        stream.reshape(2, 1, half, cols_dev), (2, n_tp, half, cols_dev)
    )
    rows = exchange(own.reshape(2 * n_tp, half, cols_dev), CTP)
    bc_flat = bc_weight.reshape(LAYERS, cols_dev, bc_width)
    packed = call(
        pack_first, shape((in_blocks + 1, cols_dev, LANES), bf16), 5, 1000000, 1000000
    )(x_weight, z_weight, bc_flat, step_weight, norm_gain)
    w_first = (packed, swap_cores(packed))
    packed = call(
        pack_rest, shape((rest, cols_dev, LANES), bf16), 6, 1000000, 1000000
    )(x_weight, z_weight, bc_flat, step_weight, out_weight, norm_gain)
    w_rest = (packed, swap_cores(packed))
    x_tap = conv_x_weight.astype(f32)
    bc_tap = conv_bc_weight.astype(f32)
    x_base = jnp.sum(conv_x_state.astype(f32) * x_tap[:, None, :-1], axis=2)
    bc_base = jnp.sum(conv_bc_state.astype(f32) * bc_tap[:, None, :-1], axis=2)
    rate = jnp.exp(decay_log)

    states_list, xconv_list, bcconv_list = [], [], []
    result = None
    hidden = None
    for l in range(LAYERS):
        if l == 0:
            hidden = rows.reshape(2, seqs, cols_dev)
            part = call(
                functools.partial(project_first, in_blocks, heads_dev),
                shape((seqs, wide), bf16), 4, 10000000, 1000000, smem=1,
            )(place, hidden, *w_first)
        else:
            part, hidden = call(
                functools.partial(project_next, in_blocks, heads_dev),
                (shape((seqs, wide), bf16), shape((2, seqs, cols_dev), bf16)), 5, 10000000, 1000000, smem=1,
            )(place, arrived, hidden, *w_rest)
        got = exchange_from_middle(part.reshape(n_z, seq_count, wide), n_z)
        got = got.astype(f32).sum(axis=0)
        tail = wide - LANES
        inv_rms = lax.rsqrt(got[:, tail + heads_dev : tail + heads_dev + 1] / MODEL_WIDTH + EPS)
        proj_x = (got[:, :x_width] * inv_rms).astype(bf16)
        proj_z = (got[:, x_width : 2 * x_width] * inv_rms).astype(bf16)
        proj_bc = (got[:, 2 * x_width : tail] * inv_rms).astype(bf16).reshape(seq_count, 2, -1)
        step_raw = got[:, tail : tail + heads_dev] * inv_rms
        inputs_x = jax.nn.silu(x_base[l] + proj_x.astype(f32) * x_tap[l, -1])
        inputs_bc = jax.nn.silu(bc_base[l] + proj_bc.astype(f32) * bc_tap[l, -1])
        b_part = inputs_bc[:, 0].reshape(seq_count, groups_dev, STATE_DIM)
        c_part = inputs_bc[:, 1].reshape(seq_count, groups_dev, STATE_DIM)
        step_size = jax.nn.softplus(step_raw + step_bias[l])
        decay_rate = jnp.exp(-step_size * rate[l])
        heads_x = inputs_x.reshape(seq_count, groups_dev, per_group, HEAD_DIM)
        step_heads = step_size.reshape(seq_count, groups_dev, per_group)
        decay_heads = decay_rate.reshape(seq_count, groups_dev, per_group)
        old_state = scan_state[l].reshape(seq_count, groups_dev, per_group, HEAD_DIM, STATE_DIM)
        state_new = (
            old_state * decay_heads[..., None, None]
            + (step_heads[..., None] * heads_x)[..., None] * b_part[:, :, None, None, :]
        )
        readout = jnp.einsum("sgepn,sgn->sgep", state_new, c_part)
        readout = (
            readout + skip_gain[l].reshape(groups_dev, per_group)[None, :, :, None] * heads_x
        )
        gated_out = readout.reshape(seq_count, -1) * jax.nn.silu(proj_z.astype(f32))
        grouped = gated_out.reshape(seq_count, groups_dev, -1)
        normed = grouped * lax.rsqrt(jnp.mean(grouped * grouped, axis=2, keepdims=True) + EPS)
        mixed_rows = (normed.reshape(seq_count, -1) * group_gain[l]).astype(bf16)
        states_list.append(state_new.reshape(seq_count, heads_dev, HEAD_DIM, STATE_DIM))
        xconv_list.append(proj_x)
        bcconv_list.append(proj_bc)

        mixed = exchange_from_middle(to_all(mixed_rows, n_z), n_z).reshape(seqs, -1)
        at = in_blocks + 1 + l * out_blocks
        if l + 1 < LAYERS:
            terms = call(
                functools.partial(mix_to_all, at, out_blocks),
                shape((n_tp, 2, seqs, cols_dev), bf16), 4, 10000000, 1000000, smem=1,
            )(place, mixed, *w_rest)
            arrived = exchange(terms, TP)
        else:
            terms = call(
                functools.partial(mix_last, at, out_blocks),
                shape((2, seqs, cols_dev), bf16), 4, 10000000, 1000000, smem=1,
            )(place, mixed, *w_rest)
            both = jnp.concatenate(
                [terms.reshape(2 * n_tp, half, cols_dev), hidden.reshape(2 * n_tp, half, cols_dev)],
                axis=1,
            )
            got = exchange(both, CTP).reshape(2, n_tp, rows_dev, cols_dev).astype(f32)
            result = got[:, :, :half].sum(axis=1) + got[:, 0, half:]
            result = result.astype(bf16).reshape(rows_dev, cols_dev)
    outs = (
        jnp.stack(states_list),
        jnp.concatenate([conv_x_state[:, :, 1:], jnp.stack(xconv_list)[:, :, None]], axis=2),
        jnp.concatenate([conv_bc_state[:, :, 1:], jnp.stack(bcconv_list)[:, :, None]], axis=2),
    )
    return (result, *outs)


def solution(mesh):
    fine = Mesh(mesh.devices.reshape(4, 4, -1, 2), ("y", "x", "z", "core"))
    dp = ("z", "core")
    in_specs = (
        P(TP, dp),
        P(None, dp),
        P(None, dp, TP),
        P(None, dp, TP),
        P(None, dp, None, TP),
        P(None, dp, None),
        P(None, None, TP),
        P(None, None, None, TP),
        P(None, TP),
        P(None, TP),
        P(None, TP),
        P(None, TP),
        P(None, TP, dp),
        P(None, dp, TP, None, None),
        P(None, dp, None, TP),
        P(None, dp, None, None, TP),
    )
    out_specs = (
        P(TP, dp),
        P(None, dp, TP, None, None),
        P(None, dp, None, TP),
        P(None, dp, None, None, TP),
    )
    return jax.shard_map(shards, mesh=fine, in_specs=in_specs, out_specs=out_specs, check_vma=False)
```

```python
import functools

import jax
import jax.numpy as jnp
from jax import lax
from jax.experimental import pallas as pl
from jax.experimental.pallas import tpu as pltpu
from jax.sharding import Mesh, PartitionSpec as P


MODEL_WIDTH = 4096
HEAD_DIM = 64
STATE_DIM = 128
LAYERS = 2
EPS = 1e-06
LANES = 128

TP = ("y", "x")
CTP = ("core", "y", "x")
VMEM = pl.BlockSpec(memory_space=pltpu.VMEM)
f32, bf16 = jnp.float32, jnp.bfloat16


def from_middle(count):
    return [(count // 2 + k) % count for k in range(count)]


def exchange_z(value, count):
    return lax.all_to_all(
        value, "z", split_axis=0, concat_axis=0, axis_index_groups=[from_middle(count)], tiled=True
    )


def exchange_plane(value, axis, sizes):
    order = [0]
    for name, size in zip(axis, sizes):
        inner = from_middle(size) if name != "core" else range(size)
        order = [at * size + k for at in order for k in inner]
    return lax.all_to_all(
        value, axis, split_axis=0, concat_axis=0, axis_index_groups=[order], tiled=True
    )


def swap_cores(value):
    return lax.ppermute(value, "core", [(0, 1), (1, 0)])


def to_all(value, count):
    return jnp.broadcast_to(value, (count, *value.shape))


def call(body, out_shape, n_in, flops, size):
    return pl.pallas_call(
        body,
        out_shape=out_shape,
        in_specs=[VMEM] * n_in,
        out_specs=jax.tree.map(lambda _: VMEM, out_shape),
        compiler_params=pltpu.CompilerParams(vmem_limit_bytes=8 * 1024 * 1024),
        cost_estimate=pl.CostEstimate(flops=flops, bytes_accessed=size, transcendentals=0),
    )


def put_projections(layer, x_ref, z_ref, bc_ref, step_ref, out_ref):
    at = 0
    for ref in (x_ref, z_ref, bc_ref, step_ref):
        for k in range(ref.shape[2] // LANES):
            out_ref[at] = ref[layer, :, k * LANES : (k + 1) * LANES]
            at += 1
    return at


def put_gain(gain, out_ref, at):
    first = gain.astype(bf16)
    left = gain - first.astype(f32)
    second = left.astype(bf16)
    third = (left - second.astype(f32)).astype(bf16)
    row = lax.broadcasted_iota(jnp.int32, (LANES, LANES), 0)
    pieces = jnp.where(row == 1, second.astype(f32), jnp.where(row == 2, third.astype(f32), 0.0))
    out_ref[at] = jnp.where(row == 0, first.astype(f32), pieces).astype(bf16)


def pack_first(x_ref, z_ref, bc_ref, step_ref, gain_ref, out_ref):
    at = put_projections(0, x_ref, z_ref, bc_ref, step_ref, out_ref)
    put_gain(gain_ref[0:1, :], out_ref, at)


def pack_rest(x_ref, z_ref, bc_ref, step_ref, w_ref, gain_ref, out_ref):
    at = put_projections(1, x_ref, z_ref, bc_ref, step_ref, out_ref)
    put_gain(gain_ref[1:2, :], out_ref, at)
    at += 1
    for l in range(LAYERS):
        for k in range(w_ref.shape[1] // LANES):
            out_ref[at] = w_ref[l, k * LANES : (k + 1) * LANES, :]
            at += 1


def swapped(rows):
    tiles = [pltpu.roll(rows[k : k + 8], 4, 0) for k in range(0, rows.shape[0], 8)]
    return jnp.concatenate(tiles, axis=0)


def project(normed, squares, first, weights, out_ref, blocks):
    total = None
    place = (lax.axis_index("y") * lax.axis_size("x") + lax.axis_index("x")) * first
    for rows, w_ref in zip(normed, weights):
        block = jnp.concatenate([w_ref[k] for k in range(blocks)], axis=1)
        term = jnp.dot(rows, block, preferred_element_type=f32)
        total = term if total is None else total + term
    wide = (blocks - 1) * LANES
    lane = lax.broadcasted_iota(jnp.int32, (total.shape[0], LANES), 1)
    tail = pltpu.roll(total[:, wide:], LANES - place, 1)
    tail = jnp.where(lane == first, squares, tail)
    out_ref[:, :wide] = total[:, :wide].astype(bf16)
    out_ref[:, wide:] = tail.astype(bf16)


def scaled(rows, w_ref, blocks):
    pieces = w_ref[blocks, :8].astype(f32)
    gain = pieces[0:1] + pieces[1:2] + pieces[2:3]
    return (rows * gain).astype(bf16)


def project_first(blocks, heads, hidden_ref, own_ref, other_ref, out_ref):
    core = lax.axis_index("core")
    rows = [hidden_ref[core], hidden_ref[1 - core]]
    wide = [swapped(r.astype(f32)) for r in rows]
    squares = jnp.sum(wide[0] * wide[0] + wide[1] * wide[1], axis=1, keepdims=True)
    weights = (own_ref, other_ref)
    normed = [scaled(r, w, blocks) for r, w in zip(wide, weights)]
    project(normed, squares, heads, weights, out_ref, blocks)


def project_next(
    blocks, heads, arrived_ref, hidden_ref, own_ref, other_ref, out_ref, next_ref
):
    core = lax.axis_index("core")
    rows = []
    weights = (own_ref, other_ref)
    for c in (core, 1 - core):
        summed = arrived_ref[0, c].astype(f32)
        for j in range(1, arrived_ref.shape[0]):
            summed = summed + arrived_ref[j, c].astype(f32)
        new = (hidden_ref[c].astype(f32) + summed).astype(bf16)
        next_ref[c] = new
        rows.append(new)
    wide = [swapped(r.astype(f32)) for r in rows]
    squares = jnp.sum(wide[0] * wide[0] + wide[1] * wide[1], axis=1, keepdims=True)
    normed = [scaled(r, w, blocks) for r, w in zip(wide, weights)]
    project(normed, squares, heads, weights, out_ref, blocks)


def out_terms(mixed_ref, w_ref, at, blocks):
    weights = jnp.concatenate([w_ref[at + k] for k in range(blocks)], axis=0)
    return swapped(jnp.dot(mixed_ref[...], weights, preferred_element_type=f32)).astype(bf16)


def mix_to_all(at, blocks, mixed_ref, own_ref, other_ref, out_ref):
    core = lax.axis_index("core")
    for c, w_ref in ((core, own_ref), (1 - core, other_ref)):
        terms = out_terms(mixed_ref, w_ref, at, blocks)
        for j in range(out_ref.shape[0]):
            out_ref[j, c] = terms


def mix_last(at, blocks, mixed_ref, own_ref, other_ref, out_ref):
    core = lax.axis_index("core")
    for c, w_ref in ((core, own_ref), (1 - core, other_ref)):
        out_ref[c] = out_terms(mixed_ref, w_ref, at, blocks)


def shards(
    stream,
    norm_gain,
    x_weight,
    z_weight,
    bc_weight,
    step_weight,
    conv_x_weight,
    conv_bc_weight,
    step_bias,
    decay_log,
    skip_gain,
    group_gain,
    out_weight,
    scan_state,
    conv_x_state,
    conv_bc_state,
):
    n_tp, n_z = lax.axis_size(TP), lax.axis_size("z")
    plane = tuple(lax.axis_size(name) for name in CTP)
    rows_dev, cols_dev = stream.shape
    half = rows_dev // 2
    seq_count, heads_dev = scan_state.shape[1:3]
    x_width = x_weight.shape[2]
    bc_width = 2 * bc_weight.shape[3]
    groups_dev = conv_bc_state.shape[4] // STATE_DIM
    per_group = heads_dev // groups_dev
    seqs = n_z * seq_count
    in_blocks = (2 * x_width + bc_width) // LANES + 1
    out_blocks = x_width // LANES
    rest = in_blocks + LAYERS * out_blocks + 1
    wide = in_blocks * LANES
    shape = jax.ShapeDtypeStruct

    own = jnp.broadcast_to(
        stream.reshape(2, 1, half, cols_dev), (2, n_tp, half, cols_dev)
    )
    rows = exchange_plane(own.reshape(2 * n_tp, half, cols_dev), CTP, plane)
    bc_flat = bc_weight.reshape(LAYERS, cols_dev, bc_width)
    packed = call(
        pack_first, shape((in_blocks + 1, cols_dev, LANES), bf16), 5, 1000000, 1000000
    )(x_weight, z_weight, bc_flat, step_weight, norm_gain)
    w_first = (packed, swap_cores(packed))
    packed = call(
        pack_rest, shape((rest, cols_dev, LANES), bf16), 6, 1000000, 1000000
    )(x_weight, z_weight, bc_flat, step_weight, out_weight, norm_gain)
    w_rest = (packed, swap_cores(packed))
    x_tap = conv_x_weight.astype(f32)
    bc_tap = conv_bc_weight.astype(f32)
    x_base = jnp.sum(conv_x_state.astype(f32) * x_tap[:, None, :-1], axis=2)
    bc_base = jnp.sum(conv_bc_state.astype(f32) * bc_tap[:, None, :-1], axis=2)
    rate = jnp.exp(decay_log)

    states_list, xconv_list, bcconv_list = [], [], []
    result = None
    hidden = None
    for l in range(LAYERS):
        if l == 0:
            hidden = rows.reshape(2, seqs, cols_dev)
            part = call(
                functools.partial(project_first, in_blocks, heads_dev),
                shape((seqs, wide), bf16), 3, 10000000, 1000000,
            )(hidden, *w_first)
        else:
            part, hidden = call(
                functools.partial(project_next, in_blocks, heads_dev),
                (shape((seqs, wide), bf16), shape((2, seqs, cols_dev), bf16)), 4, 10000000, 1000000,
            )(arrived, hidden, *w_rest)
        got = exchange_z(part.reshape(n_z, seq_count, wide), n_z)
        got = got.astype(f32).sum(axis=0)
        tail = wide - LANES
        inv_rms = lax.rsqrt(got[:, tail + heads_dev : tail + heads_dev + 1] / MODEL_WIDTH + EPS)
        proj_x = (got[:, :x_width] * inv_rms).astype(bf16)
        proj_z = (got[:, x_width : 2 * x_width] * inv_rms).astype(bf16)
        proj_bc = (got[:, 2 * x_width : tail] * inv_rms).astype(bf16).reshape(seq_count, 2, -1)
        step_raw = got[:, tail : tail + heads_dev] * inv_rms
        inputs_x = jax.nn.silu(x_base[l] + proj_x.astype(f32) * x_tap[l, -1])
        inputs_bc = jax.nn.silu(bc_base[l] + proj_bc.astype(f32) * bc_tap[l, -1])
        b_part = inputs_bc[:, 0].reshape(seq_count, groups_dev, STATE_DIM)
        c_part = inputs_bc[:, 1].reshape(seq_count, groups_dev, STATE_DIM)
        step_size = jax.nn.softplus(step_raw + step_bias[l])
        decay_rate = jnp.exp(-step_size * rate[l])
        heads_x = inputs_x.reshape(seq_count, groups_dev, per_group, HEAD_DIM)
        step_heads = step_size.reshape(seq_count, groups_dev, per_group)
        decay_heads = decay_rate.reshape(seq_count, groups_dev, per_group)
        old_state = scan_state[l].reshape(seq_count, groups_dev, per_group, HEAD_DIM, STATE_DIM)
        state_new = (
            old_state * decay_heads[..., None, None]
            + (step_heads[..., None] * heads_x)[..., None] * b_part[:, :, None, None, :]
        )
        readout = jnp.einsum("sgepn,sgn->sgep", state_new, c_part)
        readout = (
            readout + skip_gain[l].reshape(groups_dev, per_group)[None, :, :, None] * heads_x
        )
        gated_out = readout.reshape(seq_count, -1) * jax.nn.silu(proj_z.astype(f32))
        grouped = gated_out.reshape(seq_count, groups_dev, -1)
        normed = grouped * lax.rsqrt(jnp.mean(grouped * grouped, axis=2, keepdims=True) + EPS)
        mixed_rows = (normed.reshape(seq_count, -1) * group_gain[l]).astype(bf16)
        states_list.append(state_new.reshape(seq_count, heads_dev, HEAD_DIM, STATE_DIM))
        xconv_list.append(proj_x)
        bcconv_list.append(proj_bc)

        mixed = exchange_z(to_all(mixed_rows, n_z), n_z).reshape(seqs, -1)
        at = in_blocks + 1 + l * out_blocks
        if l + 1 < LAYERS:
            terms = call(
                functools.partial(mix_to_all, at, out_blocks),
                shape((n_tp, 2, seqs, cols_dev), bf16), 3, 10000000, 1000000,
            )(mixed, *w_rest)
            arrived = exchange_plane(terms, TP, plane[1:])
        else:
            terms = call(
                functools.partial(mix_last, at, out_blocks),
                shape((2, seqs, cols_dev), bf16), 3, 10000000, 1000000,
            )(mixed, *w_rest)
            both = jnp.concatenate(
                [terms.reshape(2 * n_tp, half, cols_dev), hidden.reshape(2 * n_tp, half, cols_dev)],
                axis=1,
            )
            got = exchange_plane(both, CTP, plane).reshape(2, n_tp, rows_dev, cols_dev).astype(f32)
            result = got[:, :, :half].sum(axis=1) + got[:, 0, half:]
            result = result.astype(bf16).reshape(rows_dev, cols_dev)
    outs = (
        jnp.stack(states_list),
        jnp.concatenate([conv_x_state[:, :, 1:], jnp.stack(xconv_list)[:, :, None]], axis=2),
        jnp.concatenate([conv_bc_state[:, :, 1:], jnp.stack(bcconv_list)[:, :, None]], axis=2),
    )
    return (result, *outs)


def solution(mesh):
    fine = Mesh(mesh.devices.reshape(4, 4, -1, 2), ("y", "x", "z", "core"))
    dp = ("z", "core")
    in_specs = (
        P(TP, dp),
        P(None, dp),
        P(None, dp, TP),
        P(None, dp, TP),
        P(None, dp, None, TP),
        P(None, dp, None),
        P(None, None, TP),
        P(None, None, None, TP),
        P(None, TP),
        P(None, TP),
        P(None, TP),
        P(None, TP),
        P(None, TP, dp),
        P(None, dp, TP, None, None),
        P(None, dp, None, TP),
        P(None, dp, None, None, TP),
    )
    out_specs = (
        P(TP, dp),
        P(None, dp, TP, None, None),
        P(None, dp, None, TP),
        P(None, dp, None, None, TP),
    )
    return jax.shard_map(shards, mesh=fine, in_specs=in_specs, out_specs=out_specs, check_vma=False)
```

```python
import functools

import jax
import jax.numpy as jnp
from jax import lax
from jax.experimental import pallas as pl
from jax.experimental.pallas import tpu as pltpu
from jax.sharding import Mesh, PartitionSpec as P


MODEL_WIDTH = 4096
HEAD_DIM = 64
STATE_DIM = 128
LAYERS = 2
EPS = 1e-06
LANES = 128

TP = ("y", "x")
CTP = ("core", "y", "x")
VMEM = pl.BlockSpec(memory_space=pltpu.VMEM)
f32, bf16 = jnp.float32, jnp.bfloat16


def from_middle(count):
    return [(count // 2 + k) % count for k in range(count)]


def exchange_z(value, count):
    return lax.all_to_all(
        value, "z", split_axis=0, concat_axis=0, axis_index_groups=[from_middle(count)], tiled=True
    )


def exchange_plane(value, axis, sizes):
    order = [0]
    for name, size in zip(axis, sizes):
        inner = from_middle(size) if name != "core" else range(size)
        order = [at * size + k for at in order for k in inner]
    return lax.all_to_all(
        value, axis, split_axis=0, concat_axis=0, axis_index_groups=[order], tiled=True
    )


def swap_cores(value):
    return lax.ppermute(value, "core", [(0, 1), (1, 0)])


def to_all(value, count):
    return jnp.broadcast_to(value, (count, *value.shape))


def call(body, out_shape, n_in, flops, size):
    return pl.pallas_call(
        body,
        out_shape=out_shape,
        in_specs=[VMEM] * n_in,
        out_specs=jax.tree.map(lambda _: VMEM, out_shape),
        compiler_params=pltpu.CompilerParams(vmem_limit_bytes=8 * 1024 * 1024),
        cost_estimate=pl.CostEstimate(flops=flops, bytes_accessed=size, transcendentals=0),
    )


def projection_copies(layer, x_ref, z_ref, step_ref, out_ref, sems):
    copies = []
    at = 0
    for ref in (x_ref, z_ref, None, step_ref):
        if ref is None:
            at += 2
            continue
        for k in range(ref.shape[2] // LANES):
            block = ref.at[layer, :, pl.ds(k * LANES, LANES)]
            copies.append(pltpu.make_async_copy(block, out_ref.at[at], sems.at[at]))
            at += 1
    return copies, at


def fill(layer, copies, x_ref, bc_ref, gain_ref, out_ref, gain_at, bc_buf, gain_buf, sems):
    last = sems.shape[0] - 1
    small = [
        pltpu.make_async_copy(bc_ref.at[layer], bc_buf, sems.at[last - 1]),
        pltpu.make_async_copy(gain_ref, gain_buf, sems.at[last]),
    ]
    for copy in small + copies:
        copy.start()
    small[0].wait()
    at = 2 * (x_ref.shape[2] // LANES)
    for i in range(2):
        out_ref[at + i] = bc_buf[:, i, :]
    small[1].wait()
    put_gain(gain_buf[layer : layer + 1, :], out_ref, gain_at)
    for copy in copies:
        copy.wait()


def put_gain(gain, out_ref, at):
    first = gain.astype(bf16)
    left = gain - first.astype(f32)
    second = left.astype(bf16)
    third = (left - second.astype(f32)).astype(bf16)
    row = lax.broadcasted_iota(jnp.int32, (LANES, LANES), 0)
    pieces = jnp.where(row == 1, second.astype(f32), jnp.where(row == 2, third.astype(f32), 0.0))
    out_ref[at] = jnp.where(row == 0, first.astype(f32), pieces).astype(bf16)


def pack_first(x_ref, z_ref, step_ref, bc_ref, gain_ref, out_ref, bc_buf, gain_buf, sems):
    copies, at = projection_copies(0, x_ref, z_ref, step_ref, out_ref, sems)
    fill(0, copies, x_ref, bc_ref, gain_ref, out_ref, at, bc_buf, gain_buf, sems)


def pack_rest(x_ref, z_ref, step_ref, w_ref, bc_ref, gain_ref, out_ref, bc_buf, gain_buf, sems):
    copies, gain_at = projection_copies(1, x_ref, z_ref, step_ref, out_ref, sems)
    at = gain_at + 1
    for l in range(LAYERS):
        for k in range(w_ref.shape[1] // LANES):
            block = w_ref.at[l, pl.ds(k * LANES, LANES), :]
            copies.append(pltpu.make_async_copy(block, out_ref.at[at], sems.at[at]))
            at += 1
    fill(1, copies, x_ref, bc_ref, gain_ref, out_ref, gain_at, bc_buf, gain_buf, sems)


def pack(body, count, *arrays):
    bc, gain = arrays[-2:]
    rows = bc.shape[1]
    return pl.pallas_call(
        body,
        out_shape=jax.ShapeDtypeStruct((count, rows, LANES), bf16),
        in_specs=[pl.BlockSpec(memory_space=pltpu.HBM)] * len(arrays),
        out_specs=VMEM,
        scratch_shapes=[
            pltpu.VMEM(bc.shape[1:], bf16),
            pltpu.VMEM(gain.shape, f32),
            pltpu.SemaphoreType.DMA((count + 2,)),
        ],
        compiler_params=pltpu.CompilerParams(vmem_limit_bytes=8 * 1024 * 1024),
        cost_estimate=pl.CostEstimate(flops=1000000, bytes_accessed=1000000, transcendentals=0),
    )(*(pltpu.with_memory_space_constraint(a, pltpu.HBM) for a in arrays))


def swapped(rows):
    tiles = [pltpu.roll(rows[k : k + 8], 4, 0) for k in range(0, rows.shape[0], 8)]
    return jnp.concatenate(tiles, axis=0)


def project(normed, squares, first, weights, out_ref, blocks):
    total = None
    place = (lax.axis_index("y") * lax.axis_size("x") + lax.axis_index("x")) * first
    for rows, w_ref in zip(normed, weights):
        block = jnp.concatenate([w_ref[k] for k in range(blocks)], axis=1)
        term = jnp.dot(rows, block, preferred_element_type=f32)
        total = term if total is None else total + term
    wide = (blocks - 1) * LANES
    lane = lax.broadcasted_iota(jnp.int32, (total.shape[0], LANES), 1)
    tail = pltpu.roll(total[:, wide:], LANES - place, 1)
    tail = jnp.where(lane == first, squares, tail)
    out_ref[:, :wide] = total[:, :wide].astype(bf16)
    out_ref[:, wide:] = tail.astype(bf16)


def scaled(rows, w_ref, blocks):
    pieces = w_ref[blocks, :8].astype(f32)
    gain = pieces[0:1] + pieces[1:2] + pieces[2:3]
    return (rows * gain).astype(bf16)


def project_first(blocks, heads, hidden_ref, own_ref, other_ref, out_ref):
    core = lax.axis_index("core")
    rows = [hidden_ref[core], hidden_ref[1 - core]]
    wide = [swapped(r.astype(f32)) for r in rows]
    squares = jnp.sum(wide[0] * wide[0] + wide[1] * wide[1], axis=1, keepdims=True)
    weights = (own_ref, other_ref)
    normed = [scaled(r, w, blocks) for r, w in zip(wide, weights)]
    project(normed, squares, heads, weights, out_ref, blocks)


def project_next(
    blocks, heads, arrived_ref, hidden_ref, own_ref, other_ref, out_ref, next_ref
):
    core = lax.axis_index("core")
    rows = []
    weights = (own_ref, other_ref)
    for c in (core, 1 - core):
        summed = arrived_ref[0, c].astype(f32)
        for j in range(1, arrived_ref.shape[0]):
            summed = summed + arrived_ref[j, c].astype(f32)
        new = (hidden_ref[c].astype(f32) + summed).astype(bf16)
        next_ref[c] = new
        rows.append(new)
    wide = [swapped(r.astype(f32)) for r in rows]
    squares = jnp.sum(wide[0] * wide[0] + wide[1] * wide[1], axis=1, keepdims=True)
    normed = [scaled(r, w, blocks) for r, w in zip(wide, weights)]
    project(normed, squares, heads, weights, out_ref, blocks)


def out_terms(mixed_ref, w_ref, at, blocks):
    weights = jnp.concatenate([w_ref[at + k] for k in range(blocks)], axis=0)
    return swapped(jnp.dot(mixed_ref[...], weights, preferred_element_type=f32)).astype(bf16)


def mix_to_all(at, blocks, mixed_ref, own_ref, other_ref, out_ref):
    core = lax.axis_index("core")
    for c, w_ref in ((core, own_ref), (1 - core, other_ref)):
        terms = out_terms(mixed_ref, w_ref, at, blocks)
        for j in range(out_ref.shape[0]):
            out_ref[j, c] = terms


def mix_last(at, blocks, mixed_ref, own_ref, other_ref, out_ref):
    core = lax.axis_index("core")
    for c, w_ref in ((core, own_ref), (1 - core, other_ref)):
        out_ref[c] = out_terms(mixed_ref, w_ref, at, blocks)


def shards(
    stream,
    norm_gain,
    x_weight,
    z_weight,
    bc_weight,
    step_weight,
    conv_x_weight,
    conv_bc_weight,
    step_bias,
    decay_log,
    skip_gain,
    group_gain,
    out_weight,
    scan_state,
    conv_x_state,
    conv_bc_state,
):
    n_tp, n_z = lax.axis_size(TP), lax.axis_size("z")
    plane = tuple(lax.axis_size(name) for name in CTP)
    rows_dev, cols_dev = stream.shape
    half = rows_dev // 2
    seq_count, heads_dev = scan_state.shape[1:3]
    x_width = x_weight.shape[2]
    bc_width = 2 * bc_weight.shape[3]
    groups_dev = conv_bc_state.shape[4] // STATE_DIM
    per_group = heads_dev // groups_dev
    seqs = n_z * seq_count
    in_blocks = (2 * x_width + bc_width) // LANES + 1
    out_blocks = x_width // LANES
    rest = in_blocks + LAYERS * out_blocks + 1
    wide = in_blocks * LANES
    shape = jax.ShapeDtypeStruct

    own = jnp.broadcast_to(
        stream.reshape(2, 1, half, cols_dev), (2, n_tp, half, cols_dev)
    )
    rows = exchange_plane(own.reshape(2 * n_tp, half, cols_dev), CTP, plane)
    packed = pack(
        pack_first, in_blocks + 1,
        x_weight, z_weight, step_weight, bc_weight, norm_gain,
    )
    w_first = (packed, swap_cores(packed))
    packed = pack(
        pack_rest, rest,
        x_weight, z_weight, step_weight, out_weight, bc_weight, norm_gain,
    )
    w_rest = (packed, swap_cores(packed))
    x_tap = conv_x_weight.astype(f32)
    bc_tap = conv_bc_weight.astype(f32)
    x_base = jnp.sum(conv_x_state.astype(f32) * x_tap[:, None, :-1], axis=2)
    bc_base = jnp.sum(conv_bc_state.astype(f32) * bc_tap[:, None, :-1], axis=2)
    rate = jnp.exp(decay_log)

    states_list, xconv_list, bcconv_list = [], [], []
    result = None
    hidden = None
    for l in range(LAYERS):
        if l == 0:
            hidden = rows.reshape(2, seqs, cols_dev)
            part = call(
                functools.partial(project_first, in_blocks, heads_dev),
                shape((seqs, wide), bf16), 3, 10000000, 1000000,
            )(hidden, *w_first)
        else:
            part, hidden = call(
                functools.partial(project_next, in_blocks, heads_dev),
                (shape((seqs, wide), bf16), shape((2, seqs, cols_dev), bf16)), 4, 10000000, 1000000,
            )(arrived, hidden, *w_rest)
        got = exchange_z(part.reshape(n_z, seq_count, wide), n_z)
        got = got.astype(f32).sum(axis=0)
        tail = wide - LANES
        inv_rms = lax.rsqrt(got[:, tail + heads_dev : tail + heads_dev + 1] / MODEL_WIDTH + EPS)
        proj_x = (got[:, :x_width] * inv_rms).astype(bf16)
        proj_z = (got[:, x_width : 2 * x_width] * inv_rms).astype(bf16)
        proj_bc = (got[:, 2 * x_width : tail] * inv_rms).astype(bf16).reshape(seq_count, 2, -1)
        step_raw = got[:, tail : tail + heads_dev] * inv_rms
        inputs_x = jax.nn.silu(x_base[l] + proj_x.astype(f32) * x_tap[l, -1])
        inputs_bc = jax.nn.silu(bc_base[l] + proj_bc.astype(f32) * bc_tap[l, -1])
        b_part = inputs_bc[:, 0].reshape(seq_count, groups_dev, STATE_DIM)
        c_part = inputs_bc[:, 1].reshape(seq_count, groups_dev, STATE_DIM)
        step_size = jax.nn.softplus(step_raw + step_bias[l])
        decay_rate = jnp.exp(-step_size * rate[l])
        heads_x = inputs_x.reshape(seq_count, groups_dev, per_group, HEAD_DIM)
        step_heads = step_size.reshape(seq_count, groups_dev, per_group)
        decay_heads = decay_rate.reshape(seq_count, groups_dev, per_group)
        old_state = scan_state[l].reshape(seq_count, groups_dev, per_group, HEAD_DIM, STATE_DIM)
        state_new = (
            old_state * decay_heads[..., None, None]
            + (step_heads[..., None] * heads_x)[..., None] * b_part[:, :, None, None, :]
        )
        readout = jnp.einsum("sgepn,sgn->sgep", state_new, c_part)
        readout = (
            readout + skip_gain[l].reshape(groups_dev, per_group)[None, :, :, None] * heads_x
        )
        gated_out = readout.reshape(seq_count, -1) * jax.nn.silu(proj_z.astype(f32))
        grouped = gated_out.reshape(seq_count, groups_dev, -1)
        normed = grouped * lax.rsqrt(jnp.mean(grouped * grouped, axis=2, keepdims=True) + EPS)
        mixed_rows = (normed.reshape(seq_count, -1) * group_gain[l]).astype(bf16)
        states_list.append(state_new.reshape(seq_count, heads_dev, HEAD_DIM, STATE_DIM))
        xconv_list.append(proj_x)
        bcconv_list.append(proj_bc)

        mixed = exchange_z(to_all(mixed_rows, n_z), n_z).reshape(seqs, -1)
        at = in_blocks + 1 + l * out_blocks
        if l + 1 < LAYERS:
            terms = call(
                functools.partial(mix_to_all, at, out_blocks),
                shape((n_tp, 2, seqs, cols_dev), bf16), 3, 10000000, 1000000,
            )(mixed, *w_rest)
            arrived = exchange_plane(terms, TP, plane[1:])
        else:
            terms = call(
                functools.partial(mix_last, at, out_blocks),
                shape((2, seqs, cols_dev), bf16), 3, 10000000, 1000000,
            )(mixed, *w_rest)
            both = jnp.concatenate(
                [terms.reshape(2 * n_tp, half, cols_dev), hidden.reshape(2 * n_tp, half, cols_dev)],
                axis=1,
            )
            got = exchange_plane(both, CTP, plane).reshape(2, n_tp, rows_dev, cols_dev).astype(f32)
            result = got[:, :, :half].sum(axis=1) + got[:, 0, half:]
            result = result.astype(bf16).reshape(rows_dev, cols_dev)
    outs = (
        jnp.stack(states_list),
        jnp.concatenate([conv_x_state[:, :, 1:], jnp.stack(xconv_list)[:, :, None]], axis=2),
        jnp.concatenate([conv_bc_state[:, :, 1:], jnp.stack(bcconv_list)[:, :, None]], axis=2),
    )
    return (result, *outs)


def solution(mesh):
    fine = Mesh(mesh.devices.reshape(4, 4, -1, 2), ("y", "x", "z", "core"))
    dp = ("z", "core")
    in_specs = (
        P(TP, dp),
        P(None, dp),
        P(None, dp, TP),
        P(None, dp, TP),
        P(None, dp, None, TP),
        P(None, dp, None),
        P(None, None, TP),
        P(None, None, None, TP),
        P(None, TP),
        P(None, TP),
        P(None, TP),
        P(None, TP),
        P(None, TP, dp),
        P(None, dp, TP, None, None),
        P(None, dp, None, TP),
        P(None, dp, None, None, TP),
    )
    out_specs = (
        P(TP, dp),
        P(None, dp, TP, None, None),
        P(None, dp, None, TP),
        P(None, dp, None, None, TP),
    )
    return jax.shard_map(shards, mesh=fine, in_specs=in_specs, out_specs=out_specs, check_vma=False)
```

```python
import functools

import jax
import jax.numpy as jnp
from jax import lax
from jax.experimental import pallas as pl
from jax.experimental.pallas import tpu as pltpu
from jax.sharding import Mesh, PartitionSpec as P


MODEL_WIDTH = 4096
HEAD_DIM = 64
STATE_DIM = 128
LAYERS = 2
EPS = 1e-06
LANES = 128

TP = ("y", "x")
CTP = ("core", "y", "x")
VMEM = pl.BlockSpec(memory_space=pltpu.VMEM)
f32, bf16 = jnp.float32, jnp.bfloat16


def from_middle(count):
    return [(count // 2 + k) % count for k in range(count)]


def exchange_z(value, count):
    return lax.all_to_all(
        value, "z", split_axis=0, concat_axis=0, axis_index_groups=[from_middle(count)], tiled=True
    )


def exchange_plane(value, axis, sizes):
    order = [0]
    for name, size in zip(axis, sizes):
        inner = from_middle(size) if name != "core" else range(size)
        order = [at * size + k for at in order for k in inner]
    return lax.all_to_all(
        value, axis, split_axis=0, concat_axis=0, axis_index_groups=[order], tiled=True
    )


def swap_cores(value):
    return lax.ppermute(value, "core", [(0, 1), (1, 0)])


def call(body, out_shape, n_in, flops, size):
    return pl.pallas_call(
        body,
        out_shape=out_shape,
        in_specs=[VMEM] * n_in,
        out_specs=jax.tree.map(lambda _: VMEM, out_shape),
        compiler_params=pltpu.CompilerParams(vmem_limit_bytes=8 * 1024 * 1024),
        cost_estimate=pl.CostEstimate(flops=flops, bytes_accessed=size, transcendentals=0),
    )


def projection_copies(layer, x_ref, z_ref, step_ref, out_ref, sems):
    copies = []
    at = 0
    for ref in (x_ref, z_ref, None, step_ref):
        if ref is None:
            at += 2
            continue
        for k in range(ref.shape[2] // LANES):
            block = ref.at[layer, :, pl.ds(k * LANES, LANES)]
            copies.append(pltpu.make_async_copy(block, out_ref.at[at], sems.at[at]))
            at += 1
    return copies, at


def fill(layer, copies, x_ref, bc_ref, gain_ref, out_ref, gain_at, bc_buf, gain_buf, sems):
    last = sems.shape[0] - 1
    small = [
        pltpu.make_async_copy(bc_ref.at[layer], bc_buf, sems.at[last - 1]),
        pltpu.make_async_copy(gain_ref, gain_buf, sems.at[last]),
    ]
    for copy in small + copies:
        copy.start()
    small[0].wait()
    at = 2 * (x_ref.shape[2] // LANES)
    for i in range(2):
        out_ref[at + i] = bc_buf[:, i, :]
    small[1].wait()
    put_gain(gain_buf[layer : layer + 1, :], out_ref, gain_at)
    for copy in copies:
        copy.wait()


def put_gain(gain, out_ref, at):
    first = gain.astype(bf16)
    left = gain - first.astype(f32)
    second = left.astype(bf16)
    third = (left - second.astype(f32)).astype(bf16)
    row = lax.broadcasted_iota(jnp.int32, (LANES, LANES), 0)
    pieces = jnp.where(row == 1, second.astype(f32), jnp.where(row == 2, third.astype(f32), 0.0))
    out_ref[at] = jnp.where(row == 0, first.astype(f32), pieces).astype(bf16)


def pack_first(x_ref, z_ref, step_ref, bc_ref, gain_ref, out_ref, bc_buf, gain_buf, sems):
    copies, at = projection_copies(0, x_ref, z_ref, step_ref, out_ref, sems)
    fill(0, copies, x_ref, bc_ref, gain_ref, out_ref, at, bc_buf, gain_buf, sems)


def pack_rest(x_ref, z_ref, step_ref, w_ref, bc_ref, gain_ref, out_ref, bc_buf, gain_buf, sems):
    copies, gain_at = projection_copies(1, x_ref, z_ref, step_ref, out_ref, sems)
    at = gain_at + 1
    for l in range(LAYERS):
        for k in range(w_ref.shape[1] // LANES):
            block = w_ref.at[l, pl.ds(k * LANES, LANES), :]
            copies.append(pltpu.make_async_copy(block, out_ref.at[at], sems.at[at]))
            at += 1
    fill(1, copies, x_ref, bc_ref, gain_ref, out_ref, gain_at, bc_buf, gain_buf, sems)


def pack(body, count, *arrays):
    bc, gain = arrays[-2:]
    rows = bc.shape[1]
    return pl.pallas_call(
        body,
        out_shape=jax.ShapeDtypeStruct((count, rows, LANES), bf16),
        in_specs=[pl.BlockSpec(memory_space=pltpu.HBM)] * len(arrays),
        out_specs=VMEM,
        scratch_shapes=[
            pltpu.VMEM(bc.shape[1:], bf16),
            pltpu.VMEM(gain.shape, f32),
            pltpu.SemaphoreType.DMA((count + 2,)),
        ],
        compiler_params=pltpu.CompilerParams(vmem_limit_bytes=8 * 1024 * 1024),
        cost_estimate=pl.CostEstimate(flops=1000000, bytes_accessed=1000000, transcendentals=0),
    )(*(pltpu.with_memory_space_constraint(a, pltpu.HBM) for a in arrays))


def swapped(rows):
    tiles = [pltpu.roll(rows[k : k + 8], 4, 0) for k in range(0, rows.shape[0], 8)]
    return jnp.concatenate(tiles, axis=0)


def project(normed, squares, first, weights, out_ref, blocks):
    total = None
    place = (lax.axis_index("y") * lax.axis_size("x") + lax.axis_index("x")) * first
    for rows, w_ref in zip(normed, weights):
        block = jnp.concatenate([w_ref[k] for k in range(blocks)], axis=1)
        term = jnp.dot(rows, block, preferred_element_type=f32)
        total = term if total is None else total + term
    wide = (blocks - 1) * LANES
    lane = lax.broadcasted_iota(jnp.int32, (total.shape[0], LANES), 1)
    tail = pltpu.roll(total[:, wide:], LANES - place, 1)
    tail = jnp.where(lane == first, squares, tail)
    out_ref[:, :wide] = total[:, :wide].astype(bf16)
    out_ref[:, wide:] = tail.astype(bf16)


def scaled(rows, w_ref, blocks):
    pieces = w_ref[blocks, :8].astype(f32)
    gain = pieces[0:1] + pieces[1:2] + pieces[2:3]
    return (rows * gain).astype(bf16)


def project_first(blocks, heads, hidden_ref, own_ref, other_ref, out_ref):
    core = lax.axis_index("core")
    rows = [hidden_ref[core], hidden_ref[1 - core]]
    wide = [swapped(r.astype(f32)) for r in rows]
    squares = jnp.sum(wide[0] * wide[0] + wide[1] * wide[1], axis=1, keepdims=True)
    weights = (own_ref, other_ref)
    normed = [scaled(r, w, blocks) for r, w in zip(wide, weights)]
    project(normed, squares, heads, weights, out_ref, blocks)


def project_next(
    blocks, heads, arrived_ref, hidden_ref, own_ref, other_ref, out_ref, next_ref
):
    core = lax.axis_index("core")
    rows = []
    weights = (own_ref, other_ref)
    for c in (core, 1 - core):
        summed = arrived_ref[0, c].astype(f32)
        for j in range(1, arrived_ref.shape[0]):
            summed = summed + arrived_ref[j, c].astype(f32)
        new = (hidden_ref[c].astype(f32) + summed).astype(bf16)
        next_ref[c] = new
        rows.append(new)
    wide = [swapped(r.astype(f32)) for r in rows]
    squares = jnp.sum(wide[0] * wide[0] + wide[1] * wide[1], axis=1, keepdims=True)
    normed = [scaled(r, w, blocks) for r, w in zip(wide, weights)]
    project(normed, squares, heads, weights, out_ref, blocks)


def out_terms(mixed_ref, w_ref, at, blocks):
    weights = jnp.concatenate([w_ref[at + k] for k in range(blocks)], axis=0)
    return swapped(jnp.dot(mixed_ref[...], weights, preferred_element_type=f32)).astype(bf16)


def mix_to_all(at, blocks, mixed_ref, own_ref, other_ref, out_ref):
    core = lax.axis_index("core")
    for c, w_ref in ((core, own_ref), (1 - core, other_ref)):
        terms = out_terms(mixed_ref, w_ref, at, blocks)
        for j in range(out_ref.shape[0]):
            out_ref[j, c] = terms


def mix_last(at, blocks, mixed_ref, own_ref, other_ref, out_ref):
    core = lax.axis_index("core")
    for c, w_ref in ((core, own_ref), (1 - core, other_ref)):
        out_ref[c] = out_terms(mixed_ref, w_ref, at, blocks)


def head_spread(values, head_dim, count):
    lane = lax.broadcasted_iota(jnp.int32, (values.shape[0], LANES), 1)
    pieces = []
    for k in range(count // 2):
        low = jnp.broadcast_to(values[:, 2 * k : 2 * k + 1], lane.shape)
        high = jnp.broadcast_to(values[:, 2 * k + 1 : 2 * k + 2], lane.shape)
        pieces.append(jnp.where(lane < head_dim, low, high))
    return jnp.concatenate(pieces, axis=1)


def columns(rows):
    pad = jnp.zeros((8 - rows.shape[0], rows.shape[1]), f32)
    return jnp.transpose(jnp.concatenate([rows, pad], axis=0))


def silu(v):
    return v * jax.nn.sigmoid(v)


def projected(got_ref):
    total = got_ref[0].astype(f32)
    for z in range(1, got_ref.shape[0]):
        total = total + got_ref[z].astype(f32)
    return total


def scan(layer, total, heads, par_ref, state_ref, proj_done, state_done):
    width = par_ref.shape[2]
    seqs = total.shape[0]
    tail = total[:, total.shape[1] - LANES :]
    inv = lax.rsqrt(tail[:, heads : heads + 1] / MODEL_WIDTH + EPS)
    proj = (total[:, : total.shape[1] - LANES] * inv).astype(bf16)
    proj_done(proj)
    proj = proj.astype(f32)
    par = par_ref[layer]
    inputs_x = silu(par[0:2] + proj[:, :width] * par[2:3])
    bc_width = proj.shape[1] - 2 * width
    inputs_bc = silu(par[4:6, :bc_width] + proj[:, 2 * width :] * par[6:7, :bc_width])
    raw = tail * inv + par[7:8, :LANES]
    step = jnp.maximum(raw, 0.0) + jnp.log1p(jnp.exp(-jnp.abs(raw)))
    decay = jnp.exp(-step * par[7:8, LANES : 2 * LANES])
    u_cols = columns(head_spread(step, HEAD_DIM, heads) * inputs_x)
    decay_cols = columns(head_spread(decay, HEAD_DIM, heads))
    skip = head_spread(par[7:8, 2 * LANES : 3 * LANES], HEAD_DIM, heads)
    row = lax.broadcasted_iota(jnp.int32, (8, STATE_DIM), 0)
    readouts = []
    for s in range(seqs):
        b_row = inputs_bc[s : s + 1, :STATE_DIM]
        c_row = inputs_bc[s : s + 1, STATE_DIM:]
        old = state_ref[layer, s].reshape(width, STATE_DIM)
        new = old * decay_cols[:, s : s + 1] + u_cols[:, s : s + 1] * b_row
        state_done(s, new.reshape(heads, HEAD_DIM, STATE_DIM))
        c_high = c_row.astype(bf16).astype(f32)
        c_rows = jnp.where(row == 0, c_high, jnp.where(row == 1, c_row - c_high, 0.0))
        out = lax.dot_general(
            c_rows.astype(bf16), new.astype(bf16), (((1,), (1,)), ((), ())),
            preferred_element_type=f32,
        )
        readouts.append(out[0:1] + out[1:2])
    readout = jnp.concatenate(readouts, axis=0) + skip * inputs_x
    gated = readout * silu(proj[:, width : 2 * width])
    mean = jnp.sum(gated * gated, axis=1, keepdims=True) / width
    return (gated * lax.rsqrt(mean + EPS) * par[3:4]).astype(bf16)


def scan_first(heads, got_ref, par_ref, state_ref, mixed_ref, new_ref, proj_ref):
    def proj_done(proj):
        proj_ref[...] = proj

    def state_done(s, new):
        new_ref[s] = new

    mixed = scan(0, projected(got_ref), heads, par_ref, state_ref, proj_done, state_done)
    for z in range(mixed_ref.shape[0]):
        mixed_ref[z] = mixed


def scan_last(
    heads, got_ref, par_ref, state_ref, first_ref, first_proj_ref, conv_x_ref, conv_bc_ref,
    mixed_ref, state_out, conv_x_out, conv_bc_out, new_buf, x_buf, bc_buf, sems,
):
    width = par_ref.shape[2]
    seqs = got_ref.shape[1]
    copies = [pltpu.make_async_copy(first_ref, state_out.at[0], sems.at[0])]
    copies[0].start()

    def proj_done(proj):
        x_row = lax.broadcasted_iota(jnp.int32, (4, width), 0)
        bc_row = lax.broadcasted_iota(jnp.int32, (2, STATE_DIM), 0)
        for l, source in ((0, first_proj_ref[...]), (1, proj)):
            source = source.astype(f32)
            for s in range(seqs):
                old = conv_x_ref[l, s].astype(f32)
                rows = jnp.where(x_row == 2, old[3:4], source[s : s + 1, :width])
                rows = jnp.where(x_row == 1, old[2:3], rows)
                rows = jnp.where(x_row == 0, old[1:2], rows)
                x_buf[l, s] = rows.astype(bf16)
                for k in range(3):
                    bc_buf[l, s, k] = conv_bc_ref[l, s, k + 1]
                b_row = source[s : s + 1, 2 * width : 2 * width + STATE_DIM]
                c_row = source[s : s + 1, 2 * width + STATE_DIM :]
                bc_buf[l, s, 3] = jnp.where(bc_row == 0, b_row, c_row).astype(bf16)

    def state_done(s, new):
        new_buf[s] = new
        copies.append(pltpu.make_async_copy(new_buf.at[s], state_out.at[1, s], sems.at[1 + s]))
        copies[-1].start()

    mixed = scan(1, projected(got_ref), heads, par_ref, state_ref, proj_done, state_done)
    for buf, out in ((x_buf, conv_x_out), (bc_buf, conv_bc_out)):
        copies.append(pltpu.make_async_copy(buf, out, sems.at[len(copies)]))
        copies[-1].start()
    for z in range(mixed_ref.shape[0]):
        mixed_ref[z] = mixed
    for copy in copies:
        copy.wait()


def shards(
    stream,
    norm_gain,
    x_weight,
    z_weight,
    bc_weight,
    step_weight,
    conv_x_weight,
    conv_bc_weight,
    step_bias,
    decay_log,
    skip_gain,
    group_gain,
    out_weight,
    scan_state,
    conv_x_state,
    conv_bc_state,
):
    n_tp, n_z = lax.axis_size(TP), lax.axis_size("z")
    plane = tuple(lax.axis_size(name) for name in CTP)
    rows_dev, cols_dev = stream.shape
    half = rows_dev // 2
    seq_count, heads_dev = scan_state.shape[1:3]
    x_width = x_weight.shape[2]
    bc_width = 2 * bc_weight.shape[3]
    seqs = n_z * seq_count
    in_blocks = (2 * x_width + bc_width) // LANES + 1
    out_blocks = x_width // LANES
    rest = in_blocks + LAYERS * out_blocks + 1
    wide = in_blocks * LANES
    shape = jax.ShapeDtypeStruct

    own = jnp.broadcast_to(
        stream.reshape(2, 1, half, cols_dev), (2, n_tp, half, cols_dev)
    )
    hidden = exchange_plane(own.reshape(2 * n_tp, half, cols_dev), CTP, plane)
    packed = pack(
        pack_first, in_blocks + 1,
        x_weight, z_weight, step_weight, bc_weight, norm_gain,
    )
    w_first = (packed, swap_cores(packed))
    packed = pack(
        pack_rest, rest,
        x_weight, z_weight, step_weight, out_weight, bc_weight, norm_gain,
    )
    w_rest = (packed, swap_cores(packed))
    x_tap = conv_x_weight.astype(f32)
    bc_tap = conv_bc_weight.astype(f32)
    x_base = jnp.sum(conv_x_state.astype(f32) * x_tap[:, None, :-1], axis=2)
    bc_base = jnp.sum(conv_bc_state.astype(f32) * bc_tap[:, None, :-1], axis=2)
    by_head = [
        jnp.pad(v, ((0, 0), (0, LANES - heads_dev)))
        for v in (step_bias, jnp.exp(decay_log), skip_gain)
    ]
    by_head = jnp.concatenate(by_head, axis=1)
    rows = [
        x_base,
        x_tap[:, -1:],
        group_gain[:, None],
        bc_base.reshape(LAYERS, seq_count, bc_width),
        bc_tap[:, -1].reshape(LAYERS, 1, bc_width),
        by_head[:, None],
    ]
    rows = [jnp.pad(r, ((0, 0), (0, 0), (0, x_width - r.shape[2]))) for r in rows]
    params = jnp.concatenate(rows, axis=1)

    result = None
    for l in range(LAYERS):
        if l == 0:
            hidden = hidden.reshape(2, seqs, cols_dev)
            part = call(
                functools.partial(project_first, in_blocks, heads_dev),
                shape((seqs, wide), bf16), 3, 10000000, 1000000,
            )(hidden, *w_first)
        else:
            part, hidden = call(
                functools.partial(project_next, in_blocks, heads_dev),
                (shape((seqs, wide), bf16), shape((2, seqs, cols_dev), bf16)), 4, 10000000, 1000000,
            )(arrived, hidden, *w_rest)
        got = exchange_z(part.reshape(n_z, seq_count, wide), n_z)
        mixed_shape = shape((n_z, seq_count, x_width), bf16)
        if l == 0:
            mixed, state_first, proj_first = call(
                functools.partial(scan_first, heads_dev),
                (
                    mixed_shape,
                    shape(scan_state.shape[1:], f32),
                    shape((seq_count, wide - LANES), bf16),
                ),
                3, 10000000, 1000000,
            )(got, params, scan_state)
        else:
            hbm = pl.BlockSpec(memory_space=pl.ANY)
            mixed, *outs = pl.pallas_call(
                functools.partial(scan_last, heads_dev),
                out_shape=(
                    mixed_shape,
                    shape(scan_state.shape, f32),
                    shape(conv_x_state.shape, bf16),
                    shape(conv_bc_state.shape, bf16),
                ),
                in_specs=[VMEM] * 7,
                out_specs=(VMEM, hbm, hbm, hbm),
                scratch_shapes=[
                    pltpu.VMEM(scan_state.shape[1:], f32),
                    pltpu.VMEM(conv_x_state.shape, bf16),
                    pltpu.VMEM(conv_bc_state.shape, bf16),
                    pltpu.SemaphoreType.DMA((seq_count + 3,)),
                ],
                name="scan_last",
                compiler_params=pltpu.CompilerParams(vmem_limit_bytes=8 * 1024 * 1024),
                cost_estimate=pl.CostEstimate(
                    flops=10000000, bytes_accessed=1000000, transcendentals=0
                ),
            )(got, params, scan_state, state_first, proj_first, conv_x_state, conv_bc_state)

        mixed = exchange_z(mixed, n_z).reshape(seqs, x_width)
        at = in_blocks + 1 + l * out_blocks
        if l + 1 < LAYERS:
            terms = call(
                functools.partial(mix_to_all, at, out_blocks),
                shape((n_tp, 2, seqs, cols_dev), bf16), 3, 10000000, 1000000,
            )(mixed, *w_rest)
            arrived = exchange_plane(terms, TP, plane[1:])
        else:
            terms = call(
                functools.partial(mix_last, at, out_blocks),
                shape((2, seqs, cols_dev), bf16), 3, 10000000, 1000000,
            )(mixed, *w_rest)
            both = jnp.concatenate(
                [terms.reshape(2 * n_tp, half, cols_dev), hidden.reshape(2 * n_tp, half, cols_dev)],
                axis=1,
            )
            got = exchange_plane(both, CTP, plane).reshape(2, n_tp, rows_dev, cols_dev).astype(f32)
            result = got[:, :, :half].sum(axis=1) + got[:, 0, half:]
            result = result.astype(bf16).reshape(rows_dev, cols_dev)
    return (result, *outs)


def solution(mesh):
    fine = Mesh(mesh.devices.reshape(4, 4, -1, 2), ("y", "x", "z", "core"))
    dp = ("z", "core")
    in_specs = (
        P(TP, dp),
        P(None, dp),
        P(None, dp, TP),
        P(None, dp, TP),
        P(None, dp, None, TP),
        P(None, dp, None),
        P(None, None, TP),
        P(None, None, None, TP),
        P(None, TP),
        P(None, TP),
        P(None, TP),
        P(None, TP),
        P(None, TP, dp),
        P(None, dp, TP, None, None),
        P(None, dp, None, TP),
        P(None, dp, None, None, TP),
    )
    out_specs = (
        P(TP, dp),
        P(None, dp, TP, None, None),
        P(None, dp, None, TP),
        P(None, dp, None, None, TP),
    )
    return jax.shard_map(shards, mesh=fine, in_specs=in_specs, out_specs=out_specs, check_vma=False)
```

```python
import functools

import jax
import jax.numpy as jnp
from jax import lax
from jax.experimental import pallas as pl
from jax.experimental.pallas import tpu as pltpu
from jax.sharding import Mesh, PartitionSpec as P


MODEL_WIDTH = 4096
HEAD_DIM = 64
STATE_DIM = 128
LAYERS = 2
EPS = 1e-06
LANES = 128

TP = ("y", "x")
CTP = ("core", "y", "x")
VMEM = pl.BlockSpec(memory_space=pltpu.VMEM)
f32, bf16 = jnp.float32, jnp.bfloat16


def from_middle(count):
    return [(count // 2 + k) % count for k in range(count)]


def exchange_z(value, count):
    return lax.all_to_all(
        value, "z", split_axis=0, concat_axis=0, axis_index_groups=[from_middle(count)], tiled=True
    )


def exchange_plane(value, axis, sizes):
    order = [0]
    for name, size in zip(axis, sizes):
        inner = from_middle(size) if name != "core" else range(size)
        order = [at * size + k for at in order for k in inner]
    return lax.all_to_all(
        value, axis, split_axis=0, concat_axis=0, axis_index_groups=[order], tiled=True
    )


def swap_cores(value):
    return lax.ppermute(value, "core", [(0, 1), (1, 0)])


def call(body, out_shape, n_in, flops, size):
    return pl.pallas_call(
        body,
        out_shape=out_shape,
        in_specs=[VMEM] * n_in,
        out_specs=jax.tree.map(lambda _: VMEM, out_shape),
        compiler_params=pltpu.CompilerParams(vmem_limit_bytes=8 * 1024 * 1024),
        cost_estimate=pl.CostEstimate(flops=flops, bytes_accessed=size, transcendentals=0),
    )


def projection_copies(layer, x_ref, z_ref, step_ref, out_ref, sems):
    copies = []
    at = 0
    for ref in (x_ref, z_ref, None, step_ref):
        if ref is None:
            at += 2
            continue
        for k in range(ref.shape[2] // LANES):
            block = ref.at[layer, :, pl.ds(k * LANES, LANES)]
            copies.append(pltpu.make_async_copy(block, out_ref.at[at], sems.at[at]))
            at += 1
    return copies, at


def start_small(layer, bc_ref, gain_ref, bc_buf, gain_buf, sems):
    last = sems.shape[0] - 1
    small = [
        pltpu.make_async_copy(bc_ref.at[layer], bc_buf, sems.at[last - 1]),
        pltpu.make_async_copy(gain_ref, gain_buf, sems.at[last]),
    ]
    for copy in small:
        copy.start()
    return small


def finish(layer, small, copies, x_ref, out_ref, gain_at, bc_buf, gain_buf):
    small[0].wait()
    at = 2 * (x_ref.shape[2] // LANES)
    for i in range(2):
        out_ref[at + i] = bc_buf[:, i, :]
    small[1].wait()
    put_gain(gain_buf[layer : layer + 1, :], out_ref, gain_at)
    for copy in copies:
        copy.wait()


def put_gain(gain, out_ref, at):
    first = gain.astype(bf16)
    left = gain - first.astype(f32)
    second = left.astype(bf16)
    third = (left - second.astype(f32)).astype(bf16)
    row = lax.broadcasted_iota(jnp.int32, (LANES, LANES), 0)
    pieces = jnp.where(row == 1, second.astype(f32), jnp.where(row == 2, third.astype(f32), 0.0))
    out_ref[at] = jnp.where(row == 0, first.astype(f32), pieces).astype(bf16)


def enter(
    stream_ref, x_ref, z_ref, step_ref, bc_ref, gain_ref,
    own_out, out_ref, stream_buf, own_buf, bc_buf, gain_buf, sems,
):
    copies, at = projection_copies(0, x_ref, z_ref, step_ref, out_ref, sems)
    count = sems.shape[0]
    into = pltpu.make_async_copy(stream_ref, stream_buf, sems.at[count - 4])
    into.start()
    small = start_small(0, bc_ref, gain_ref, bc_buf, gain_buf, sems)
    for copy in copies:
        copy.start()
    into.wait()
    half = own_buf.shape[1]
    each = own_buf.shape[0] // 2
    for c in range(2):
        rows = stream_buf[c * half : (c + 1) * half]
        for p in range(each):
            own_buf[c * each + p] = rows
    out = pltpu.make_async_copy(own_buf, own_out, sems.at[count - 3])
    out.start()
    finish(0, small, copies + [out], x_ref, out_ref, at, bc_buf, gain_buf)


def pack_rest(
    x_ref, z_ref, step_ref, w_ref, bc_ref, gain_ref,
    tap_x_ref, tap_bc_ref, bias_ref, decay_ref, skip_ref, group_ref, conv_x_ref, conv_bc_ref,
    out_ref, par_ref, bc_buf, gain_buf,
    tap_x, tap_bc, bias, decay, skip, group, conv_x, conv_bc, sems, par_sems,
):
    sources = (tap_x_ref, tap_bc_ref, bias_ref, decay_ref, skip_ref, group_ref)
    sources += (conv_x_ref, conv_bc_ref)
    bufs = (tap_x, tap_bc, bias, decay, skip, group, conv_x, conv_bc)
    loads = [
        pltpu.make_async_copy(a, b, par_sems.at[k]) for k, (a, b) in enumerate(zip(sources, bufs))
    ]
    copies, gain_at = projection_copies(1, x_ref, z_ref, step_ref, out_ref, sems)
    at = gain_at + 1
    for l in range(LAYERS):
        for k in range(w_ref.shape[1] // LANES):
            block = w_ref.at[l, pl.ds(k * LANES, LANES), :]
            copies.append(pltpu.make_async_copy(block, out_ref.at[at], sems.at[at]))
            at += 1
    for copy in loads:
        copy.start()
    small = start_small(1, bc_ref, gain_ref, bc_buf, gain_buf, sems)
    for copy in copies:
        copy.start()
    for copy in loads:
        copy.wait()
    heads = bias.shape[1]
    seqs = conv_x.shape[1]
    taps = tap_x.shape[0] - 1
    par_ref[...] = jnp.zeros(par_ref.shape, f32)
    for l in range(LAYERS):
        for s in range(seqs):
            old = conv_x[l, s].astype(f32)
            base = jnp.zeros((1, old.shape[1]), f32)
            pair = jnp.zeros((2, LANES), f32)
            for k in range(taps):
                base = base + old[k : k + 1] * tap_x[k].astype(f32)[l : l + 1]
                pair = pair + conv_bc[l, s, k].astype(f32) * tap_bc[l, k].astype(f32)
            par_ref[l, s : s + 1, :] = base
            par_ref[l, 4 + s : 5 + s, :LANES] = pair[0:1]
            par_ref[l, 4 + s : 5 + s, LANES : 2 * LANES] = pair[1:2]
        last = tap_bc[l, taps].astype(f32)
        par_ref[l, 2:3, :] = tap_x[taps].astype(f32)[l : l + 1]
        par_ref[l, 3:4, :] = group[l : l + 1, :]
        par_ref[l, 6:7, :LANES] = last[0:1]
        par_ref[l, 6:7, LANES : 2 * LANES] = last[1:2]
        par_ref[l, 7:8, :heads] = bias[l : l + 1, :]
        par_ref[l, 7:8, LANES : LANES + heads] = jnp.exp(decay[l : l + 1, :])
        par_ref[l, 7:8, 2 * LANES : 2 * LANES + heads] = skip[l : l + 1, :]
    finish(1, small, copies, x_ref, out_ref, gain_at, bc_buf, gain_buf)


def pack(body, out_shape, out_specs, scratch, *arrays):
    return pl.pallas_call(
        body,
        out_shape=out_shape,
        in_specs=[pl.BlockSpec(memory_space=pltpu.HBM)] * len(arrays),
        out_specs=out_specs,
        scratch_shapes=scratch,
        compiler_params=pltpu.CompilerParams(vmem_limit_bytes=8 * 1024 * 1024),
        cost_estimate=pl.CostEstimate(flops=1000000, bytes_accessed=1000000, transcendentals=0),
    )(*(pltpu.with_memory_space_constraint(a, pltpu.HBM) for a in arrays))


def swapped(rows):
    tiles = [pltpu.roll(rows[k : k + 8], 4, 0) for k in range(0, rows.shape[0], 8)]
    return jnp.concatenate(tiles, axis=0)


def project(normed, squares, first, weights, out_ref, blocks):
    total = None
    place = (lax.axis_index("y") * lax.axis_size("x") + lax.axis_index("x")) * first
    for rows, w_ref in zip(normed, weights):
        block = jnp.concatenate([w_ref[k] for k in range(blocks)], axis=1)
        term = jnp.dot(rows, block, preferred_element_type=f32)
        total = term if total is None else total + term
    wide = (blocks - 1) * LANES
    lane = lax.broadcasted_iota(jnp.int32, (total.shape[0], LANES), 1)
    tail = pltpu.roll(total[:, wide:], LANES - place, 1)
    tail = jnp.where(lane == first, squares, tail)
    out_ref[:, :wide] = total[:, :wide].astype(bf16)
    out_ref[:, wide:] = tail.astype(bf16)


def scaled(rows, w_ref, blocks):
    pieces = w_ref[blocks, :8].astype(f32)
    gain = pieces[0:1] + pieces[1:2] + pieces[2:3]
    return (rows * gain).astype(bf16)


def project_first(blocks, heads, hidden_ref, own_ref, other_ref, out_ref):
    core = lax.axis_index("core")
    rows = [hidden_ref[core], hidden_ref[1 - core]]
    wide = [swapped(r.astype(f32)) for r in rows]
    squares = jnp.sum(wide[0] * wide[0] + wide[1] * wide[1], axis=1, keepdims=True)
    weights = (own_ref, other_ref)
    normed = [scaled(r, w, blocks) for r, w in zip(wide, weights)]
    project(normed, squares, heads, weights, out_ref, blocks)


def project_next(
    blocks, heads, arrived_ref, hidden_ref, own_ref, other_ref, out_ref, next_ref
):
    core = lax.axis_index("core")
    rows = []
    weights = (own_ref, other_ref)
    for c in (core, 1 - core):
        summed = arrived_ref[0, c].astype(f32)
        for j in range(1, arrived_ref.shape[0]):
            summed = summed + arrived_ref[j, c].astype(f32)
        new = (hidden_ref[c].astype(f32) + summed).astype(bf16)
        next_ref[c] = new
        rows.append(new)
    wide = [swapped(r.astype(f32)) for r in rows]
    squares = jnp.sum(wide[0] * wide[0] + wide[1] * wide[1], axis=1, keepdims=True)
    normed = [scaled(r, w, blocks) for r, w in zip(wide, weights)]
    project(normed, squares, heads, weights, out_ref, blocks)


def out_terms(mixed_ref, w_ref, at, blocks):
    weights = jnp.concatenate([w_ref[at + k] for k in range(blocks)], axis=0)
    return swapped(jnp.dot(mixed_ref[...], weights, preferred_element_type=f32)).astype(bf16)


def mix_to_all(at, blocks, mixed_ref, own_ref, other_ref, out_ref):
    core = lax.axis_index("core")
    for c, w_ref in ((core, own_ref), (1 - core, other_ref)):
        terms = out_terms(mixed_ref, w_ref, at, blocks)
        for j in range(out_ref.shape[0]):
            out_ref[j, c] = terms


def mix_last(at, blocks, mixed_ref, own_ref, other_ref, out_ref):
    core = lax.axis_index("core")
    for c, w_ref in ((core, own_ref), (1 - core, other_ref)):
        out_ref[c] = out_terms(mixed_ref, w_ref, at, blocks)


def head_spread(values, head_dim, count):
    lane = lax.broadcasted_iota(jnp.int32, (values.shape[0], LANES), 1)
    pieces = []
    for k in range(count // 2):
        low = jnp.broadcast_to(values[:, 2 * k : 2 * k + 1], lane.shape)
        high = jnp.broadcast_to(values[:, 2 * k + 1 : 2 * k + 2], lane.shape)
        pieces.append(jnp.where(lane < head_dim, low, high))
    return jnp.concatenate(pieces, axis=1)


def columns(rows):
    pad = jnp.zeros((8 - rows.shape[0], rows.shape[1]), f32)
    return jnp.transpose(jnp.concatenate([rows, pad], axis=0))


def silu(v):
    return v * jax.nn.sigmoid(v)


def projected(got_ref):
    total = got_ref[0].astype(f32)
    for z in range(1, got_ref.shape[0]):
        total = total + got_ref[z].astype(f32)
    return total


def scan(layer, total, heads, par_ref, state_ref, proj_done, state_done):
    width = par_ref.shape[2]
    seqs = total.shape[0]
    tail = total[:, total.shape[1] - LANES :]
    inv = lax.rsqrt(tail[:, heads : heads + 1] / MODEL_WIDTH + EPS)
    proj = (total[:, : total.shape[1] - LANES] * inv).astype(bf16)
    proj_done(proj)
    proj = proj.astype(f32)
    par = par_ref[layer]
    inputs_x = silu(par[0:2] + proj[:, :width] * par[2:3])
    bc_width = proj.shape[1] - 2 * width
    inputs_bc = silu(par[4:6, :bc_width] + proj[:, 2 * width :] * par[6:7, :bc_width])
    raw = tail * inv + par[7:8, :LANES]
    step = jnp.maximum(raw, 0.0) + jnp.log1p(jnp.exp(-jnp.abs(raw)))
    decay = jnp.exp(-step * par[7:8, LANES : 2 * LANES])
    u_cols = columns(head_spread(step, HEAD_DIM, heads) * inputs_x)
    decay_cols = columns(head_spread(decay, HEAD_DIM, heads))
    skip = head_spread(par[7:8, 2 * LANES : 3 * LANES], HEAD_DIM, heads)
    row = lax.broadcasted_iota(jnp.int32, (8, STATE_DIM), 0)
    readouts = []
    for s in range(seqs):
        b_row = inputs_bc[s : s + 1, :STATE_DIM]
        c_row = inputs_bc[s : s + 1, STATE_DIM:]
        old = state_ref[layer, s].reshape(width, STATE_DIM)
        new = old * decay_cols[:, s : s + 1] + u_cols[:, s : s + 1] * b_row
        state_done(s, new.reshape(heads, HEAD_DIM, STATE_DIM))
        c_high = c_row.astype(bf16).astype(f32)
        c_rows = jnp.where(row == 0, c_high, jnp.where(row == 1, c_row - c_high, 0.0))
        out = lax.dot_general(
            c_rows.astype(bf16), new.astype(bf16), (((1,), (1,)), ((), ())),
            preferred_element_type=f32,
        )
        readouts.append(out[0:1] + out[1:2])
    readout = jnp.concatenate(readouts, axis=0) + skip * inputs_x
    gated = readout * silu(proj[:, width : 2 * width])
    mean = jnp.sum(gated * gated, axis=1, keepdims=True) / width
    return (gated * lax.rsqrt(mean + EPS) * par[3:4]).astype(bf16)


def scan_first(heads, got_ref, par_ref, state_ref, mixed_ref, new_ref, proj_ref):
    def proj_done(proj):
        proj_ref[...] = proj

    def state_done(s, new):
        new_ref[s] = new

    mixed = scan(0, projected(got_ref), heads, par_ref, state_ref, proj_done, state_done)
    for z in range(mixed_ref.shape[0]):
        mixed_ref[z] = mixed


def scan_last(
    heads, got_ref, par_ref, state_ref, first_ref, first_proj_ref, conv_x_ref, conv_bc_ref,
    mixed_ref, state_out, conv_x_out, conv_bc_out, new_buf, x_buf, bc_buf, sems,
):
    width = par_ref.shape[2]
    seqs = got_ref.shape[1]
    copies = [pltpu.make_async_copy(first_ref, state_out.at[0], sems.at[0])]
    copies[0].start()

    def proj_done(proj):
        x_row = lax.broadcasted_iota(jnp.int32, (4, width), 0)
        bc_row = lax.broadcasted_iota(jnp.int32, (2, STATE_DIM), 0)
        for l, source in ((0, first_proj_ref[...]), (1, proj)):
            source = source.astype(f32)
            for s in range(seqs):
                old = conv_x_ref[l, s].astype(f32)
                rows = jnp.where(x_row == 2, old[3:4], source[s : s + 1, :width])
                rows = jnp.where(x_row == 1, old[2:3], rows)
                rows = jnp.where(x_row == 0, old[1:2], rows)
                x_buf[l, s] = rows.astype(bf16)
                for k in range(3):
                    bc_buf[l, s, k] = conv_bc_ref[l, s, k + 1]
                b_row = source[s : s + 1, 2 * width : 2 * width + STATE_DIM]
                c_row = source[s : s + 1, 2 * width + STATE_DIM :]
                bc_buf[l, s, 3] = jnp.where(bc_row == 0, b_row, c_row).astype(bf16)

    def state_done(s, new):
        new_buf[s] = new
        copies.append(pltpu.make_async_copy(new_buf.at[s], state_out.at[1, s], sems.at[1 + s]))
        copies[-1].start()

    mixed = scan(1, projected(got_ref), heads, par_ref, state_ref, proj_done, state_done)
    for buf, out in ((x_buf, conv_x_out), (bc_buf, conv_bc_out)):
        copies.append(pltpu.make_async_copy(buf, out, sems.at[len(copies)]))
        copies[-1].start()
    for z in range(mixed_ref.shape[0]):
        mixed_ref[z] = mixed
    for copy in copies:
        copy.wait()


def shards(
    stream,
    norm_gain,
    x_weight,
    z_weight,
    bc_weight,
    step_weight,
    conv_x_weight,
    conv_bc_weight,
    step_bias,
    decay_log,
    skip_gain,
    group_gain,
    out_weight,
    scan_state,
    conv_x_state,
    conv_bc_state,
):
    n_tp, n_z = lax.axis_size(TP), lax.axis_size("z")
    plane = tuple(lax.axis_size(name) for name in CTP)
    rows_dev, cols_dev = stream.shape
    half = rows_dev // 2
    seq_count, heads_dev = scan_state.shape[1:3]
    x_width = x_weight.shape[2]
    bc_width = 2 * bc_weight.shape[3]
    seqs = n_z * seq_count
    in_blocks = (2 * x_width + bc_width) // LANES + 1
    out_blocks = x_width // LANES
    rest = in_blocks + LAYERS * out_blocks + 1
    wide = in_blocks * LANES
    shape = jax.ShapeDtypeStruct

    dma = pltpu.SemaphoreType.DMA
    shared = [pltpu.VMEM(bc_weight.shape[1:], bf16), pltpu.VMEM(norm_gain.shape, f32)]
    own, packed = pack(
        enter,
        (shape((2 * n_tp, half, cols_dev), bf16), shape((in_blocks + 1, cols_dev, LANES), bf16)),
        (pl.BlockSpec(memory_space=pl.ANY), VMEM),
        [
            pltpu.VMEM(stream.shape, bf16),
            pltpu.VMEM((2 * n_tp, half, cols_dev), bf16),
            *shared,
            dma((in_blocks + 4,)),
        ],
        stream, x_weight, z_weight, step_weight, bc_weight, norm_gain,
    )
    hidden = exchange_plane(own, CTP, plane)
    w_first = (packed, swap_cores(packed))
    small = (
        jnp.transpose(conv_x_weight, (1, 0, 2)), conv_bc_weight, step_bias, decay_log,
        skip_gain, group_gain, conv_x_state, conv_bc_state,
    )
    packed, params = pack(
        pack_rest,
        (shape((rest, cols_dev, LANES), bf16), shape((LAYERS, 8, x_width), f32)),
        (VMEM, VMEM),
        [
            *shared,
            *(pltpu.VMEM(a.shape, a.dtype) for a in small),
            dma((rest + 2,)),
            dma((len(small),)),
        ],
        x_weight, z_weight, step_weight, out_weight, bc_weight, norm_gain, *small,
    )
    w_rest = (packed, swap_cores(packed))

    result = None
    for l in range(LAYERS):
        if l == 0:
            hidden = hidden.reshape(2, seqs, cols_dev)
            part = call(
                functools.partial(project_first, in_blocks, heads_dev),
                shape((seqs, wide), bf16), 3, 10000000, 1000000,
            )(hidden, *w_first)
        else:
            part, hidden = call(
                functools.partial(project_next, in_blocks, heads_dev),
                (shape((seqs, wide), bf16), shape((2, seqs, cols_dev), bf16)), 4, 10000000, 1000000,
            )(arrived, hidden, *w_rest)
        got = exchange_z(part.reshape(n_z, seq_count, wide), n_z)
        mixed_shape = shape((n_z, seq_count, x_width), bf16)
        if l == 0:
            mixed, state_first, proj_first = call(
                functools.partial(scan_first, heads_dev),
                (
                    mixed_shape,
                    shape(scan_state.shape[1:], f32),
                    shape((seq_count, wide - LANES), bf16),
                ),
                3, 10000000, 1000000,
            )(got, params, scan_state)
        else:
            hbm = pl.BlockSpec(memory_space=pl.ANY)
            mixed, *outs = pl.pallas_call(
                functools.partial(scan_last, heads_dev),
                out_shape=(
                    mixed_shape,
                    shape(scan_state.shape, f32),
                    shape(conv_x_state.shape, bf16),
                    shape(conv_bc_state.shape, bf16),
                ),
                in_specs=[VMEM] * 7,
                out_specs=(VMEM, hbm, hbm, hbm),
                scratch_shapes=[
                    pltpu.VMEM(scan_state.shape[1:], f32),
                    pltpu.VMEM(conv_x_state.shape, bf16),
                    pltpu.VMEM(conv_bc_state.shape, bf16),
                    pltpu.SemaphoreType.DMA((seq_count + 3,)),
                ],
                name="scan_last",
                compiler_params=pltpu.CompilerParams(vmem_limit_bytes=8 * 1024 * 1024),
                cost_estimate=pl.CostEstimate(
                    flops=10000000, bytes_accessed=1000000, transcendentals=0
                ),
            )(got, params, scan_state, state_first, proj_first, conv_x_state, conv_bc_state)

        mixed = exchange_z(mixed, n_z).reshape(seqs, x_width)
        at = in_blocks + 1 + l * out_blocks
        if l + 1 < LAYERS:
            terms = call(
                functools.partial(mix_to_all, at, out_blocks),
                shape((n_tp, 2, seqs, cols_dev), bf16), 3, 10000000, 1000000,
            )(mixed, *w_rest)
            arrived = exchange_plane(terms, TP, plane[1:])
        else:
            terms = call(
                functools.partial(mix_last, at, out_blocks),
                shape((2, seqs, cols_dev), bf16), 3, 10000000, 1000000,
            )(mixed, *w_rest)
            both = jnp.concatenate(
                [terms.reshape(2 * n_tp, half, cols_dev), hidden.reshape(2 * n_tp, half, cols_dev)],
                axis=1,
            )
            got = exchange_plane(both, CTP, plane).reshape(2, n_tp, rows_dev, cols_dev).astype(f32)
            result = got[:, :, :half].sum(axis=1) + got[:, 0, half:]
            result = result.astype(bf16).reshape(rows_dev, cols_dev)
    return (result, *outs)


def solution(mesh):
    fine = Mesh(mesh.devices.reshape(4, 4, -1, 2), ("y", "x", "z", "core"))
    dp = ("z", "core")
    in_specs = (
        P(TP, dp),
        P(None, dp),
        P(None, dp, TP),
        P(None, dp, TP),
        P(None, dp, None, TP),
        P(None, dp, None),
        P(None, None, TP),
        P(None, None, None, TP),
        P(None, TP),
        P(None, TP),
        P(None, TP),
        P(None, TP),
        P(None, TP, dp),
        P(None, dp, TP, None, None),
        P(None, dp, None, TP),
        P(None, dp, None, None, TP),
    )
    out_specs = (
        P(TP, dp),
        P(None, dp, TP, None, None),
        P(None, dp, None, TP),
        P(None, dp, None, None, TP),
    )
    return jax.shard_map(shards, mesh=fine, in_specs=in_specs, out_specs=out_specs, check_vma=False)
```

```python
import functools

import jax
import jax.numpy as jnp
from jax import lax
from jax.experimental import pallas as pl
from jax.experimental.pallas import tpu as pltpu
from jax.sharding import Mesh, PartitionSpec as P


MODEL_WIDTH = 4096
HEAD_DIM = 64
STATE_DIM = 128
LAYERS = 2
EPS = 1e-06
LANES = 128

TP = ("y", "x")
CTP = ("core", "y", "x")
VMEM = pl.BlockSpec(memory_space=pltpu.VMEM)
f32, bf16 = jnp.float32, jnp.bfloat16


def from_middle(count):
    return [(count // 2 + k) % count for k in range(count)]


def exchange_z(value, count):
    return lax.all_to_all(
        value, "z", split_axis=0, concat_axis=0, axis_index_groups=[from_middle(count)], tiled=True
    )


def exchange_plane(value, axis, sizes):
    order = [0]
    for name, size in zip(axis, sizes):
        inner = from_middle(size) if name != "core" else range(size)
        order = [at * size + k for at in order for k in inner]
    return lax.all_to_all(
        value, axis, split_axis=0, concat_axis=0, axis_index_groups=[order], tiled=True
    )


def swap_cores(value):
    return lax.ppermute(value, "core", [(0, 1), (1, 0)])


def call(body, out_shape, n_in, flops, size):
    return pl.pallas_call(
        body,
        out_shape=out_shape,
        in_specs=[VMEM] * n_in,
        out_specs=jax.tree.map(lambda _: VMEM, out_shape),
        compiler_params=pltpu.CompilerParams(vmem_limit_bytes=8 * 1024 * 1024),
        cost_estimate=pl.CostEstimate(flops=flops, bytes_accessed=size, transcendentals=0),
    )


def span(at, count=1):
    return pl.ds(at * LANES, count * LANES)


def projection_copies(layer, x_ref, z_ref, step_ref, out_ref, sems):
    copies = []
    at = 0
    for ref in (x_ref, z_ref, None, step_ref):
        if ref is None:
            at += 2
            continue
        count = ref.shape[2] // LANES
        target = out_ref.at[:, span(at, count)]
        copies.append(pltpu.make_async_copy(ref.at[layer], target, sems.at[at]))
        at += count
    return copies, at


def put_pair(both, out_ref, at):
    rows = both.shape[0]
    to = lax.broadcasted_iota(jnp.int32, (rows, rows), 0)
    source = lax.broadcasted_iota(jnp.int32, (rows, rows), 1)
    want = 2 * (to % (rows // 2)) + to // (rows // 2)
    pick = jnp.where(source == want, 1.0, 0.0).astype(bf16)
    parted = jnp.dot(pick, both, preferred_element_type=f32).astype(bf16)
    out_ref[:, span(at)] = parted[: rows // 2]
    out_ref[:, span(at + 1)] = parted[rows // 2 :]


def put_gain(gain, out_ref, at):
    first = gain.astype(bf16)
    left = gain - first.astype(f32)
    second = left.astype(bf16)
    third = (left - second.astype(f32)).astype(bf16)
    row = lax.broadcasted_iota(jnp.int32, (LANES, LANES), 0)
    pieces = jnp.where(row == 1, second.astype(f32), jnp.where(row == 2, third.astype(f32), 0.0))
    out_ref[:, span(at)] = jnp.where(row == 0, first.astype(f32), pieces).astype(bf16)


def enter(
    stream_ref, x_ref, z_ref, step_ref, w_ref, bc_ref, gain_ref,
    tap_x_ref, tap_bc_ref, bias_ref, decay_ref, skip_ref, group_ref, conv_x_ref, conv_bc_ref,
    own_out, out_ref, rest_ref, par_ref,
    stream_buf, own_buf, bc_buf, gain_buf,
    tap_x, tap_bc, bias, decay, skip, group, conv_x, conv_bc, sems, rest_sems, par_sems,
):
    into = pltpu.make_async_copy(stream_ref, stream_buf, par_sems.at[0])
    into.start()
    sources = (tap_x_ref, tap_bc_ref, bias_ref, decay_ref, skip_ref, group_ref)
    sources += (conv_x_ref, conv_bc_ref, bc_ref, gain_ref)
    bufs = (tap_x, tap_bc, bias, decay, skip, group, conv_x, conv_bc, bc_buf, gain_buf)
    loads = [
        pltpu.make_async_copy(a, b, par_sems.at[2 + k])
        for k, (a, b) in enumerate(zip(sources, bufs))
    ]
    for copy in loads[-2:]:
        copy.start()
    copies, gain_at = projection_copies(0, x_ref, z_ref, step_ref, out_ref, sems)
    others, _ = projection_copies(1, x_ref, z_ref, step_ref, rest_ref, rest_sems)
    at = gain_at + 1
    for l in range(LAYERS):
        for k in range(w_ref.shape[1] // LANES):
            block = w_ref.at[l, pl.ds(k * LANES, LANES), :]
            others.append(pltpu.make_async_copy(block, rest_ref.at[:, span(at)], rest_sems.at[at]))
            at += 1
    for copy in copies + loads[:-2] + others:
        copy.start()
    into.wait()
    half = own_buf.shape[1]
    each = own_buf.shape[0] // 2
    for c in range(2):
        rows = stream_buf[c * half : (c + 1) * half]
        for p in range(each):
            own_buf[c * each + p] = rows
    out = pltpu.make_async_copy(own_buf, own_out, par_sems.at[1])
    out.start()
    for copy in loads:
        copy.wait()
    shared_at = 2 * (x_ref.shape[2] // LANES)
    for l, ref in ((0, out_ref), (1, rest_ref)):
        put_pair(bc_buf[l], ref, shared_at)
        put_gain(gain_buf[l : l + 1, :], ref, gain_at)
    heads = bias.shape[1]
    seqs = conv_x.shape[1]
    taps = tap_x.shape[0] - 1
    par_ref[...] = jnp.zeros(par_ref.shape, f32)
    for l in range(LAYERS):
        for s in range(seqs):
            old = conv_x[l, s].astype(f32)
            base = jnp.zeros((1, old.shape[1]), f32)
            pair = jnp.zeros((2, LANES), f32)
            for k in range(taps):
                base = base + old[k : k + 1] * tap_x[k].astype(f32)[l : l + 1]
                pair = pair + conv_bc[l, s, k].astype(f32) * tap_bc[l, k].astype(f32)
            par_ref[l, s : s + 1, :] = base
            par_ref[l, 4 + s : 5 + s, :LANES] = pair[0:1]
            par_ref[l, 4 + s : 5 + s, LANES : 2 * LANES] = pair[1:2]
        last = tap_bc[l, taps].astype(f32)
        par_ref[l, 2:3, :] = tap_x[taps].astype(f32)[l : l + 1]
        par_ref[l, 3:4, :] = group[l : l + 1, :]
        par_ref[l, 6:7, :LANES] = last[0:1]
        par_ref[l, 6:7, LANES : 2 * LANES] = last[1:2]
        par_ref[l, 7:8, :heads] = bias[l : l + 1, :]
        par_ref[l, 7:8, LANES : LANES + heads] = jnp.exp(decay[l : l + 1, :])
        par_ref[l, 7:8, 2 * LANES : 2 * LANES + heads] = skip[l : l + 1, :]
    for copy in copies + others + [out]:
        copy.wait()


def pack(body, out_shape, out_specs, scratch, *arrays):
    return pl.pallas_call(
        body,
        out_shape=out_shape,
        in_specs=[pl.BlockSpec(memory_space=pltpu.HBM)] * len(arrays),
        out_specs=out_specs,
        scratch_shapes=scratch,
        compiler_params=pltpu.CompilerParams(vmem_limit_bytes=8 * 1024 * 1024),
        cost_estimate=pl.CostEstimate(flops=1000000, bytes_accessed=1000000, transcendentals=0),
    )(*(pltpu.with_memory_space_constraint(a, pltpu.HBM) for a in arrays))


def swapped(rows):
    tiles = [pltpu.roll(rows[k : k + 8], 4, 0) for k in range(0, rows.shape[0], 8)]
    return jnp.concatenate(tiles, axis=0)


def project(normed, squares, first, weights, out_ref, blocks):
    total = None
    place = (lax.axis_index("y") * lax.axis_size("x") + lax.axis_index("x")) * first
    for rows, w_ref in zip(normed, weights):
        block = w_ref[:, : blocks * LANES]
        term = jnp.dot(rows, block, preferred_element_type=f32)
        total = term if total is None else total + term
    wide = (blocks - 1) * LANES
    lane = lax.broadcasted_iota(jnp.int32, (total.shape[0], LANES), 1)
    tail = pltpu.roll(total[:, wide:], LANES - place, 1)
    tail = jnp.where(lane == first, squares, tail)
    out_ref[:, :wide] = total[:, :wide].astype(bf16)
    out_ref[:, wide:] = tail.astype(bf16)


def scaled(rows, w_ref, blocks):
    pieces = w_ref[:8, span(blocks)].astype(f32)
    gain = pieces[0:1] + pieces[1:2] + pieces[2:3]
    return (rows * gain).astype(bf16)


def project_first(blocks, heads, hidden_ref, own_ref, other_ref, out_ref):
    core = lax.axis_index("core")
    rows = [hidden_ref[core], hidden_ref[1 - core]]
    wide = [swapped(r.astype(f32)) for r in rows]
    squares = jnp.sum(wide[0] * wide[0] + wide[1] * wide[1], axis=1, keepdims=True)
    weights = (own_ref, other_ref)
    normed = [scaled(r, w, blocks) for r, w in zip(wide, weights)]
    project(normed, squares, heads, weights, out_ref, blocks)


def project_next(
    blocks, heads, arrived_ref, hidden_ref, own_ref, other_ref, out_ref, next_ref
):
    core = lax.axis_index("core")
    rows = []
    weights = (own_ref, other_ref)
    for c in (core, 1 - core):
        summed = arrived_ref[0, c].astype(f32)
        for j in range(1, arrived_ref.shape[0]):
            summed = summed + arrived_ref[j, c].astype(f32)
        new = (hidden_ref[c].astype(f32) + summed).astype(bf16)
        next_ref[c] = new
        rows.append(new)
    wide = [swapped(r.astype(f32)) for r in rows]
    squares = jnp.sum(wide[0] * wide[0] + wide[1] * wide[1], axis=1, keepdims=True)
    normed = [scaled(r, w, blocks) for r, w in zip(wide, weights)]
    project(normed, squares, heads, weights, out_ref, blocks)


def out_terms(mixed_ref, w_ref, at, blocks):
    weights = jnp.concatenate([w_ref[:, span(at + k)] for k in range(blocks)], axis=0)
    return swapped(jnp.dot(mixed_ref[...], weights, preferred_element_type=f32)).astype(bf16)


def mix_to_all(at, blocks, mixed_ref, own_ref, other_ref, out_ref):
    core = lax.axis_index("core")
    for c, w_ref in ((core, own_ref), (1 - core, other_ref)):
        terms = out_terms(mixed_ref, w_ref, at, blocks)
        for j in range(out_ref.shape[0]):
            out_ref[j, c] = terms


def mix_last(at, blocks, mixed_ref, own_ref, other_ref, out_ref):
    core = lax.axis_index("core")
    for c, w_ref in ((core, own_ref), (1 - core, other_ref)):
        out_ref[c] = out_terms(mixed_ref, w_ref, at, blocks)


def head_spread(values, head_dim, count):
    lane = lax.broadcasted_iota(jnp.int32, (values.shape[0], LANES), 1)
    pieces = []
    for k in range(count // 2):
        low = jnp.broadcast_to(values[:, 2 * k : 2 * k + 1], lane.shape)
        high = jnp.broadcast_to(values[:, 2 * k + 1 : 2 * k + 2], lane.shape)
        pieces.append(jnp.where(lane < head_dim, low, high))
    return jnp.concatenate(pieces, axis=1)


def columns(rows):
    pad = jnp.zeros((8 - rows.shape[0], rows.shape[1]), f32)
    return jnp.transpose(jnp.concatenate([rows, pad], axis=0))


def silu(v):
    return v * jax.nn.sigmoid(v)


def projected(got_ref):
    total = got_ref[0].astype(f32)
    for z in range(1, got_ref.shape[0]):
        total = total + got_ref[z].astype(f32)
    return total


def scan(layer, total, heads, par_ref, state_ref, proj_done, state_done):
    width = par_ref.shape[2]
    seqs = total.shape[0]
    tail = total[:, total.shape[1] - LANES :]
    inv = lax.rsqrt(tail[:, heads : heads + 1] / MODEL_WIDTH + EPS)
    rounded = (total[:, : total.shape[1] - LANES] * inv).astype(bf16)
    proj = rounded.astype(f32)
    par = par_ref[layer]
    inputs_x = silu(par[0:2] + proj[:, :width] * par[2:3])
    bc_width = proj.shape[1] - 2 * width
    inputs_bc = silu(par[4:6, :bc_width] + proj[:, 2 * width :] * par[6:7, :bc_width])
    raw = tail * inv + par[7:8, :LANES]
    step = jnp.maximum(raw, 0.0) + jnp.log1p(jnp.exp(-jnp.abs(raw)))
    decay = jnp.exp(-step * par[7:8, LANES : 2 * LANES])
    u_rows = head_spread(step, HEAD_DIM, heads) * inputs_x
    u_cols = columns(u_rows)
    row = lax.broadcasted_iota(jnp.int32, (8, STATE_DIM), 0)
    b_rows, c_rows = inputs_bc[:, :STATE_DIM], inputs_bc[:, STATE_DIM:]
    reads = []
    for s in range(seqs):
        c_row = c_rows[s : s + 1]
        c_high = c_row.astype(bf16).astype(f32)
        c_both = jnp.where(row == 0, c_high, jnp.where(row == 1, c_row - c_high, 0.0))
        old = state_ref[layer, s].reshape(width, STATE_DIM)
        out = lax.dot_general(
            c_both.astype(bf16), old.astype(bf16), (((1,), (1,)), ((), ())),
            preferred_element_type=f32,
        )
        reads.append(out[0:1] + out[1:2])
    for s in range(seqs):
        new = []
        for h in range(heads):
            at = h * HEAD_DIM
            keep = jnp.broadcast_to(decay[s : s + 1, h : h + 1], (HEAD_DIM, STATE_DIM))
            add = u_cols[at : at + HEAD_DIM, s : s + 1] * b_rows[s : s + 1]
            new.append(state_ref[layer, s, h] * keep + add)
        state_done(s, new)
    proj_done(rounded)
    readout = head_spread(decay, HEAD_DIM, heads) * jnp.concatenate(reads, axis=0)
    readout = readout + u_rows * jnp.sum(b_rows * c_rows, axis=1, keepdims=True)
    readout = readout + head_spread(par[7:8, 2 * LANES : 3 * LANES], HEAD_DIM, heads) * inputs_x
    gated = readout * silu(proj[:, width : 2 * width])
    mean = jnp.sum(gated * gated, axis=1, keepdims=True) / width
    return (gated * lax.rsqrt(mean + EPS) * par[3:4]).astype(bf16)


def scan_first(heads, got_ref, par_ref, state_ref, mixed_ref, new_ref, proj_ref):
    def proj_done(proj):
        proj_ref[...] = proj

    def state_done(s, new):
        for h in range(heads):
            new_ref[s, h] = new[h]

    mixed = scan(0, projected(got_ref), heads, par_ref, state_ref, proj_done, state_done)
    for z in range(mixed_ref.shape[0]):
        mixed_ref[z] = mixed


def scan_last(
    heads, got_ref, par_ref, state_ref, first_ref, first_proj_ref, conv_x_ref, conv_bc_ref,
    mixed_ref, state_out, conv_x_out, conv_bc_out, new_buf, x_buf, bc_buf, sems,
):
    width = par_ref.shape[2]
    seqs = got_ref.shape[1]
    copies = [pltpu.make_async_copy(first_ref, state_out.at[0], sems.at[0])]
    copies[0].start()

    def proj_done(proj):
        x_row = lax.broadcasted_iota(jnp.int32, (4, width), 0)
        bc_row = lax.broadcasted_iota(jnp.int32, (2, STATE_DIM), 0)
        for l, source in ((0, first_proj_ref[...]), (1, proj)):
            source = source.astype(f32)
            for s in range(seqs):
                old = conv_x_ref[l, s].astype(f32)
                rows = jnp.where(x_row == 2, old[3:4], source[s : s + 1, :width])
                rows = jnp.where(x_row == 1, old[2:3], rows)
                rows = jnp.where(x_row == 0, old[1:2], rows)
                x_buf[l, s] = rows.astype(bf16)
                for k in range(3):
                    bc_buf[l, s, k] = conv_bc_ref[l, s, k + 1]
                b_row = source[s : s + 1, 2 * width : 2 * width + STATE_DIM]
                c_row = source[s : s + 1, 2 * width + STATE_DIM :]
                bc_buf[l, s, 3] = jnp.where(bc_row == 0, b_row, c_row).astype(bf16)

    def state_done(s, new):
        for h in range(heads):
            new_buf[s, h] = new[h]
        copies.append(pltpu.make_async_copy(new_buf.at[s], state_out.at[1, s], sems.at[1 + s]))
        copies[-1].start()

    mixed = scan(1, projected(got_ref), heads, par_ref, state_ref, proj_done, state_done)
    for buf, out in ((x_buf, conv_x_out), (bc_buf, conv_bc_out)):
        copies.append(pltpu.make_async_copy(buf, out, sems.at[len(copies)]))
        copies[-1].start()
    for z in range(mixed_ref.shape[0]):
        mixed_ref[z] = mixed
    for copy in copies:
        copy.wait()


def shards(
    stream,
    norm_gain,
    x_weight,
    z_weight,
    bc_weight,
    step_weight,
    conv_x_weight,
    conv_bc_weight,
    step_bias,
    decay_log,
    skip_gain,
    group_gain,
    out_weight,
    scan_state,
    conv_x_state,
    conv_bc_state,
):
    n_tp, n_z = lax.axis_size(TP), lax.axis_size("z")
    plane = tuple(lax.axis_size(name) for name in CTP)
    rows_dev, cols_dev = stream.shape
    half = rows_dev // 2
    seq_count, heads_dev = scan_state.shape[1:3]
    x_width = x_weight.shape[2]
    bc_width = 2 * bc_weight.shape[3]
    seqs = n_z * seq_count
    in_blocks = (2 * x_width + bc_width) // LANES + 1
    out_blocks = x_width // LANES
    rest = in_blocks + LAYERS * out_blocks + 1
    wide = in_blocks * LANES
    shape = jax.ShapeDtypeStruct

    dma = pltpu.SemaphoreType.DMA
    bc_rows = bc_weight.reshape(LAYERS, 2 * cols_dev, LANES)
    small = (
        jnp.transpose(conv_x_weight, (1, 0, 2)), conv_bc_weight, step_bias, decay_log,
        skip_gain, group_gain, conv_x_state, conv_bc_state,
    )
    own, packed, packed_rest, params = pack(
        enter,
        (
            shape((2 * n_tp, half, cols_dev), bf16),
            shape((cols_dev, (in_blocks + 1) * LANES), bf16),
            shape((cols_dev, rest * LANES), bf16),
            shape((LAYERS, 8, x_width), f32),
        ),
        (pl.BlockSpec(memory_space=pl.ANY), VMEM, VMEM, VMEM),
        [
            pltpu.VMEM(stream.shape, bf16),
            pltpu.VMEM((2 * n_tp, half, cols_dev), bf16),
            pltpu.VMEM(bc_rows.shape, bf16),
            pltpu.VMEM(norm_gain.shape, f32),
            *(pltpu.VMEM(a.shape, a.dtype) for a in small),
            dma((in_blocks + 1,)),
            dma((rest,)),
            dma((len(small) + 4,)),
        ],
        stream, x_weight, z_weight, step_weight, out_weight, bc_rows, norm_gain, *small,
    )
    hidden = exchange_plane(own, CTP, plane)
    w_first = (packed, swap_cores(packed))
    w_rest = (packed_rest, swap_cores(packed_rest))

    result = None
    for l in range(LAYERS):
        if l == 0:
            hidden = hidden.reshape(2, seqs, cols_dev)
            part = call(
                functools.partial(project_first, in_blocks, heads_dev),
                shape((seqs, wide), bf16), 3, 10000000, 1000000,
            )(hidden, *w_first)
        else:
            part, hidden = call(
                functools.partial(project_next, in_blocks, heads_dev),
                (shape((seqs, wide), bf16), shape((2, seqs, cols_dev), bf16)), 4, 10000000, 1000000,
            )(arrived, hidden, *w_rest)
        got = exchange_z(part.reshape(n_z, seq_count, wide), n_z)
        mixed_shape = shape((n_z, seq_count, x_width), bf16)
        if l == 0:
            mixed, state_first, proj_first = call(
                functools.partial(scan_first, heads_dev),
                (
                    mixed_shape,
                    shape(scan_state.shape[1:], f32),
                    shape((seq_count, wide - LANES), bf16),
                ),
                3, 10000000, 1000000,
            )(got, params, scan_state)
        else:
            hbm = pl.BlockSpec(memory_space=pl.ANY)
            mixed, *outs = pl.pallas_call(
                functools.partial(scan_last, heads_dev),
                out_shape=(
                    mixed_shape,
                    shape(scan_state.shape, f32),
                    shape(conv_x_state.shape, bf16),
                    shape(conv_bc_state.shape, bf16),
                ),
                in_specs=[VMEM] * 7,
                out_specs=(VMEM, hbm, hbm, hbm),
                scratch_shapes=[
                    pltpu.VMEM(scan_state.shape[1:], f32),
                    pltpu.VMEM(conv_x_state.shape, bf16),
                    pltpu.VMEM(conv_bc_state.shape, bf16),
                    pltpu.SemaphoreType.DMA((seq_count + 3,)),
                ],
                name="scan_last",
                compiler_params=pltpu.CompilerParams(vmem_limit_bytes=8 * 1024 * 1024),
                cost_estimate=pl.CostEstimate(
                    flops=10000000, bytes_accessed=1000000, transcendentals=0
                ),
            )(got, params, scan_state, state_first, proj_first, conv_x_state, conv_bc_state)

        mixed = exchange_z(mixed, n_z).reshape(seqs, x_width)
        at = in_blocks + 1 + l * out_blocks
        if l + 1 < LAYERS:
            terms = call(
                functools.partial(mix_to_all, at, out_blocks),
                shape((n_tp, 2, seqs, cols_dev), bf16), 3, 10000000, 1000000,
            )(mixed, *w_rest)
            arrived = exchange_plane(terms, TP, plane[1:])
        else:
            terms = call(
                functools.partial(mix_last, at, out_blocks),
                shape((2, seqs, cols_dev), bf16), 3, 10000000, 1000000,
            )(mixed, *w_rest)
            both = jnp.concatenate(
                [terms.reshape(2 * n_tp, half, cols_dev), hidden.reshape(2 * n_tp, half, cols_dev)],
                axis=1,
            )
            got = exchange_plane(both, CTP, plane).reshape(2, n_tp, rows_dev, cols_dev).astype(f32)
            result = got[:, :, :half].sum(axis=1) + got[:, 0, half:]
            result = result.astype(bf16).reshape(rows_dev, cols_dev)
    return (result, *outs)


def solution(mesh):
    fine = Mesh(mesh.devices.reshape(4, 4, -1, 2), ("y", "x", "z", "core"))
    dp = ("z", "core")
    in_specs = (
        P(TP, dp),
        P(None, dp),
        P(None, dp, TP),
        P(None, dp, TP),
        P(None, dp, None, TP),
        P(None, dp, None),
        P(None, None, TP),
        P(None, None, None, TP),
        P(None, TP),
        P(None, TP),
        P(None, TP),
        P(None, TP),
        P(None, TP, dp),
        P(None, dp, TP, None, None),
        P(None, dp, None, TP),
        P(None, dp, None, None, TP),
    )
    out_specs = (
        P(TP, dp),
        P(None, dp, TP, None, None),
        P(None, dp, None, TP),
        P(None, dp, None, None, TP),
    )
    return jax.shard_map(shards, mesh=fine, in_specs=in_specs, out_specs=out_specs, check_vma=False)
```

```python
import functools

import jax
import jax.numpy as jnp
from jax import lax
from jax.experimental import pallas as pl
from jax.experimental.pallas import tpu as pltpu
from jax.sharding import Mesh, PartitionSpec as P


MODEL_WIDTH = 4096
HEAD_DIM = 64
STATE_DIM = 128
LAYERS = 2
EPS = 1e-06
LANES = 128

TP = ("y", "x")
CTP = ("core", "y", "x")
VMEM = pl.BlockSpec(memory_space=pltpu.VMEM)
f32, bf16 = jnp.float32, jnp.bfloat16


def from_middle(count):
    return [(count // 2 + k) % count for k in range(count)]


def exchange_z(value, count):
    return lax.all_to_all(
        value, "z", split_axis=0, concat_axis=0, axis_index_groups=[from_middle(count)], tiled=True
    )


def exchange_plane(value, axis, sizes):
    order = [0]
    for name, size in zip(axis, sizes):
        inner = from_middle(size)
        order = [at * size + k for at in order for k in inner]
    return lax.all_to_all(
        value, axis, split_axis=0, concat_axis=0, axis_index_groups=[order], tiled=True
    )


def swap_cores(value):
    return lax.ppermute(value, "core", [(0, 1), (1, 0)])


def call(body, out_shape, n_in, flops, size):
    return pl.pallas_call(
        body,
        out_shape=out_shape,
        in_specs=[VMEM] * n_in,
        out_specs=jax.tree.map(lambda _: VMEM, out_shape),
        compiler_params=pltpu.CompilerParams(vmem_limit_bytes=8 * 1024 * 1024),
        cost_estimate=pl.CostEstimate(flops=flops, bytes_accessed=size, transcendentals=0),
    )


def span(at, count=1):
    return pl.ds(at * LANES, count * LANES)


def projection_copies(layer, x_ref, z_ref, step_ref, out_ref, sems):
    copies = []
    at = 0
    for ref in (x_ref, z_ref, None, step_ref):
        if ref is None:
            at += 2
            continue
        count = ref.shape[2] // LANES
        target = out_ref.at[:, span(at, count)]
        copies.append(pltpu.make_async_copy(ref.at[layer], target, sems.at[at]))
        at += count
    return copies, at


def put_pair(both, out_ref, at):
    rows = both.shape[0]
    to = lax.broadcasted_iota(jnp.int32, (rows, rows), 0)
    source = lax.broadcasted_iota(jnp.int32, (rows, rows), 1)
    want = 2 * (to % (rows // 2)) + to // (rows // 2)
    pick = jnp.where(source == want, 1.0, 0.0).astype(bf16)
    parted = jnp.dot(pick, both, preferred_element_type=f32).astype(bf16)
    out_ref[:, span(at)] = parted[: rows // 2]
    out_ref[:, span(at + 1)] = parted[rows // 2 :]


def put_gain(gain, out_ref, at):
    first = gain.astype(bf16)
    left = gain - first.astype(f32)
    second = left.astype(bf16)
    third = (left - second.astype(f32)).astype(bf16)
    row = lax.broadcasted_iota(jnp.int32, (LANES, LANES), 0)
    pieces = jnp.where(row == 1, second.astype(f32), jnp.where(row == 2, third.astype(f32), 0.0))
    out_ref[:, span(at)] = jnp.where(row == 0, first.astype(f32), pieces).astype(bf16)


def enter(
    stream_ref, x_ref, z_ref, step_ref, w_ref, bc_ref, gain_ref,
    tap_x_ref, tap_bc_ref, bias_ref, decay_ref, skip_ref, group_ref, conv_x_ref, conv_bc_ref,
    own_out, out_ref, rest_ref, par_ref,
    stream_buf, own_buf, bc_buf, gain_buf,
    tap_x, tap_bc, bias, decay, skip, group, conv_x, conv_bc, sems, rest_sems, par_sems,
):
    into = pltpu.make_async_copy(stream_ref, stream_buf, par_sems.at[0])
    into.start()
    sources = (tap_x_ref, tap_bc_ref, bias_ref, decay_ref, skip_ref, group_ref)
    sources += (conv_x_ref, conv_bc_ref, bc_ref, gain_ref)
    bufs = (tap_x, tap_bc, bias, decay, skip, group, conv_x, conv_bc, bc_buf, gain_buf)
    loads = [
        pltpu.make_async_copy(a, b, par_sems.at[2 + k])
        for k, (a, b) in enumerate(zip(sources, bufs))
    ]
    for copy in loads[-2:]:
        copy.start()
    copies, gain_at = projection_copies(0, x_ref, z_ref, step_ref, out_ref, sems)
    others, _ = projection_copies(1, x_ref, z_ref, step_ref, rest_ref, rest_sems)
    at = gain_at + 1
    for l in range(LAYERS):
        for k in range(w_ref.shape[1] // LANES):
            block = w_ref.at[l, pl.ds(k * LANES, LANES), :]
            others.append(pltpu.make_async_copy(block, rest_ref.at[:, span(at)], rest_sems.at[at]))
            at += 1
    for copy in copies + loads[:-2] + others:
        copy.start()
    into.wait()
    half = own_buf.shape[1]
    each = own_buf.shape[0] // 2
    for c in range(2):
        rows = stream_buf[(1 - c) * half : (2 - c) * half]
        for p in range(each):
            own_buf[c * each + p] = rows
    out = pltpu.make_async_copy(own_buf, own_out, par_sems.at[1])
    out.start()
    for copy in loads:
        copy.wait()
    shared_at = 2 * (x_ref.shape[2] // LANES)
    for l, ref in ((0, out_ref), (1, rest_ref)):
        put_pair(bc_buf[l], ref, shared_at)
        put_gain(gain_buf[l : l + 1, :], ref, gain_at)
    heads = bias.shape[1]
    seqs = conv_x.shape[1]
    taps = tap_x.shape[0] - 1
    par_ref[...] = jnp.zeros(par_ref.shape, f32)
    for l in range(LAYERS):
        for s in range(seqs):
            old = conv_x[l, s].astype(f32)
            base = jnp.zeros((1, old.shape[1]), f32)
            pair = jnp.zeros((2, LANES), f32)
            for k in range(taps):
                base = base + old[k : k + 1] * tap_x[k].astype(f32)[l : l + 1]
                pair = pair + conv_bc[l, s, k].astype(f32) * tap_bc[l, k].astype(f32)
            par_ref[l, s : s + 1, :] = base
            par_ref[l, 4 + s : 5 + s, :LANES] = pair[0:1]
            par_ref[l, 4 + s : 5 + s, LANES : 2 * LANES] = pair[1:2]
        last = tap_bc[l, taps].astype(f32)
        par_ref[l, 2:3, :] = tap_x[taps].astype(f32)[l : l + 1]
        par_ref[l, 3:4, :] = group[l : l + 1, :]
        par_ref[l, 6:7, :LANES] = last[0:1]
        par_ref[l, 6:7, LANES : 2 * LANES] = last[1:2]
        par_ref[l, 7:8, :heads] = bias[l : l + 1, :]
        par_ref[l, 7:8, LANES : LANES + heads] = jnp.exp(decay[l : l + 1, :])
        par_ref[l, 7:8, 2 * LANES : 2 * LANES + heads] = skip[l : l + 1, :]
    for copy in copies + others + [out]:
        copy.wait()


def pack(body, out_shape, out_specs, scratch, *arrays):
    return pl.pallas_call(
        body,
        out_shape=out_shape,
        in_specs=[pl.BlockSpec(memory_space=pltpu.HBM)] * len(arrays),
        out_specs=out_specs,
        scratch_shapes=scratch,
        compiler_params=pltpu.CompilerParams(vmem_limit_bytes=8 * 1024 * 1024),
        cost_estimate=pl.CostEstimate(flops=1000000, bytes_accessed=1000000, transcendentals=0),
    )(*(pltpu.with_memory_space_constraint(a, pltpu.HBM) for a in arrays))


def swapped(rows):
    tiles = [pltpu.roll(rows[k : k + 8], 4, 0) for k in range(0, rows.shape[0], 8)]
    return jnp.concatenate(tiles, axis=0)


def project(normed, squares, first, weights, out_ref, blocks):
    total = None
    place = (lax.axis_index("y") * lax.axis_size("x") + lax.axis_index("x")) * first
    for rows, w_ref in zip(normed, weights):
        block = w_ref[:, : blocks * LANES]
        term = jnp.dot(rows, block, preferred_element_type=f32)
        total = term if total is None else total + term
    wide = (blocks - 1) * LANES
    lane = lax.broadcasted_iota(jnp.int32, (total.shape[0], LANES), 1)
    tail = pltpu.roll(total[:, wide:], LANES - place, 1)
    tail = jnp.where(lane == first, squares, tail)
    out_ref[:, :wide] = total[:, :wide].astype(bf16)
    out_ref[:, wide:] = tail.astype(bf16)


def scaled(rows, w_ref, blocks):
    pieces = w_ref[:8, span(blocks)].astype(f32)
    gain = pieces[0:1] + pieces[1:2] + pieces[2:3]
    return (rows * gain).astype(bf16)


def project_first(blocks, heads, hidden_ref, own_ref, other_ref, out_ref):
    core = 1 - lax.axis_index("core")
    rows = [hidden_ref[core], hidden_ref[1 - core]]
    wide = [swapped(r.astype(f32)) for r in rows]
    squares = jnp.sum(wide[0] * wide[0] + wide[1] * wide[1], axis=1, keepdims=True)
    weights = (own_ref, other_ref)
    normed = [scaled(r, w, blocks) for r, w in zip(wide, weights)]
    project(normed, squares, heads, weights, out_ref, blocks)


def project_next(
    blocks, heads, arrived_ref, hidden_ref, own_ref, other_ref, out_ref, next_ref
):
    core = 1 - lax.axis_index("core")
    rows = []
    weights = (own_ref, other_ref)
    for c in (core, 1 - core):
        summed = arrived_ref[0, c].astype(f32)
        for j in range(1, arrived_ref.shape[0]):
            summed = summed + arrived_ref[j, c].astype(f32)
        new = (hidden_ref[c].astype(f32) + summed).astype(bf16)
        next_ref[c] = new
        rows.append(new)
    wide = [swapped(r.astype(f32)) for r in rows]
    squares = jnp.sum(wide[0] * wide[0] + wide[1] * wide[1], axis=1, keepdims=True)
    normed = [scaled(r, w, blocks) for r, w in zip(wide, weights)]
    project(normed, squares, heads, weights, out_ref, blocks)


def out_terms(mixed_ref, w_ref, at, blocks):
    weights = jnp.concatenate([w_ref[:, span(at + k)] for k in range(blocks)], axis=0)
    return swapped(jnp.dot(mixed_ref[...], weights, preferred_element_type=f32)).astype(bf16)


def mix_to_all(at, blocks, mixed_ref, own_ref, other_ref, out_ref):
    core = 1 - lax.axis_index("core")
    for c, w_ref in ((core, own_ref), (1 - core, other_ref)):
        terms = out_terms(mixed_ref, w_ref, at, blocks)
        for j in range(out_ref.shape[0]):
            out_ref[j, c] = terms


def mix_last(at, blocks, mixed_ref, own_ref, other_ref, out_ref):
    core = 1 - lax.axis_index("core")
    for c, w_ref in ((core, own_ref), (1 - core, other_ref)):
        out_ref[c] = out_terms(mixed_ref, w_ref, at, blocks)


def head_spread(values, head_dim, count):
    lane = lax.broadcasted_iota(jnp.int32, (values.shape[0], LANES), 1)
    pieces = []
    for k in range(count // 2):
        low = jnp.broadcast_to(values[:, 2 * k : 2 * k + 1], lane.shape)
        high = jnp.broadcast_to(values[:, 2 * k + 1 : 2 * k + 2], lane.shape)
        pieces.append(jnp.where(lane < head_dim, low, high))
    return jnp.concatenate(pieces, axis=1)


def columns(rows):
    pad = jnp.zeros((8 - rows.shape[0], rows.shape[1]), f32)
    return jnp.transpose(jnp.concatenate([rows, pad], axis=0))


def silu(v):
    return v * jax.nn.sigmoid(v)


def projected(got_ref):
    total = got_ref[0].astype(f32)
    for z in range(1, got_ref.shape[0]):
        total = total + got_ref[z].astype(f32)
    return total


def scan(layer, total, heads, par_ref, state_ref, proj_done, state_done):
    width = par_ref.shape[2]
    seqs = total.shape[0]
    tail = total[:, total.shape[1] - LANES :]
    inv = lax.rsqrt(tail[:, heads : heads + 1] / MODEL_WIDTH + EPS)
    rounded = (total[:, : total.shape[1] - LANES] * inv).astype(bf16)
    proj = rounded.astype(f32)
    par = par_ref[layer]
    inputs_x = silu(par[0:2] + proj[:, :width] * par[2:3])
    bc_width = proj.shape[1] - 2 * width
    inputs_bc = silu(par[4:6, :bc_width] + proj[:, 2 * width :] * par[6:7, :bc_width])
    raw = tail * inv + par[7:8, :LANES]
    step = jnp.maximum(raw, 0.0) + jnp.log1p(jnp.exp(-jnp.abs(raw)))
    decay = jnp.exp(-step * par[7:8, LANES : 2 * LANES])
    u_rows = head_spread(step, HEAD_DIM, heads) * inputs_x
    u_cols = columns(u_rows)
    row = lax.broadcasted_iota(jnp.int32, (8, STATE_DIM), 0)
    b_rows, c_rows = inputs_bc[:, :STATE_DIM], inputs_bc[:, STATE_DIM:]
    reads = []
    for s in range(seqs):
        c_row = c_rows[s : s + 1]
        c_high = c_row.astype(bf16).astype(f32)
        c_both = jnp.where(row == 0, c_high, jnp.where(row == 1, c_row - c_high, 0.0))
        old = state_ref[layer, s].reshape(width, STATE_DIM)
        out = lax.dot_general(
            c_both.astype(bf16), old.astype(bf16), (((1,), (1,)), ((), ())),
            preferred_element_type=f32,
        )
        reads.append(out[0:1] + out[1:2])
    for s in range(seqs):
        new = []
        for h in range(heads):
            at = h * HEAD_DIM
            keep = jnp.broadcast_to(decay[s : s + 1, h : h + 1], (HEAD_DIM, STATE_DIM))
            add = u_cols[at : at + HEAD_DIM, s : s + 1] * b_rows[s : s + 1]
            new.append(state_ref[layer, s, h] * keep + add)
        state_done(s, new)
    proj_done(rounded)
    readout = head_spread(decay, HEAD_DIM, heads) * jnp.concatenate(reads, axis=0)
    readout = readout + u_rows * jnp.sum(b_rows * c_rows, axis=1, keepdims=True)
    readout = readout + head_spread(par[7:8, 2 * LANES : 3 * LANES], HEAD_DIM, heads) * inputs_x
    gated = readout * silu(proj[:, width : 2 * width])
    mean = jnp.sum(gated * gated, axis=1, keepdims=True) / width
    return (gated * lax.rsqrt(mean + EPS) * par[3:4]).astype(bf16)


def scan_first(heads, got_ref, par_ref, state_ref, mixed_ref, new_ref, proj_ref):
    def proj_done(proj):
        proj_ref[...] = proj

    def state_done(s, new):
        for h in range(heads):
            new_ref[s, h] = new[h]

    mixed = scan(0, projected(got_ref), heads, par_ref, state_ref, proj_done, state_done)
    for z in range(mixed_ref.shape[0]):
        mixed_ref[z] = mixed


def scan_last(
    heads, got_ref, par_ref, state_ref, first_ref, first_proj_ref, conv_x_ref, conv_bc_ref,
    mixed_ref, state_out, conv_x_out, conv_bc_out, new_buf, x_buf, bc_buf, sems,
):
    width = par_ref.shape[2]
    seqs = got_ref.shape[1]
    copies = [pltpu.make_async_copy(first_ref, state_out.at[0], sems.at[0])]
    copies[0].start()

    def proj_done(proj):
        x_row = lax.broadcasted_iota(jnp.int32, (4, width), 0)
        bc_row = lax.broadcasted_iota(jnp.int32, (2, STATE_DIM), 0)
        for l, source in ((0, first_proj_ref[...]), (1, proj)):
            source = source.astype(f32)
            for s in range(seqs):
                old = conv_x_ref[l, s].astype(f32)
                rows = jnp.where(x_row == 2, old[3:4], source[s : s + 1, :width])
                rows = jnp.where(x_row == 1, old[2:3], rows)
                rows = jnp.where(x_row == 0, old[1:2], rows)
                x_buf[l, s] = rows.astype(bf16)
                for k in range(3):
                    bc_buf[l, s, k] = conv_bc_ref[l, s, k + 1]
                b_row = source[s : s + 1, 2 * width : 2 * width + STATE_DIM]
                c_row = source[s : s + 1, 2 * width + STATE_DIM :]
                bc_buf[l, s, 3] = jnp.where(bc_row == 0, b_row, c_row).astype(bf16)

    def state_done(s, new):
        for h in range(heads):
            new_buf[s, h] = new[h]
        copies.append(pltpu.make_async_copy(new_buf.at[s], state_out.at[1, s], sems.at[1 + s]))
        copies[-1].start()

    mixed = scan(1, projected(got_ref), heads, par_ref, state_ref, proj_done, state_done)
    for buf, out in ((x_buf, conv_x_out), (bc_buf, conv_bc_out)):
        copies.append(pltpu.make_async_copy(buf, out, sems.at[len(copies)]))
        copies[-1].start()
    for z in range(mixed_ref.shape[0]):
        mixed_ref[z] = mixed
    for copy in copies:
        copy.wait()


def shards(
    stream,
    norm_gain,
    x_weight,
    z_weight,
    bc_weight,
    step_weight,
    conv_x_weight,
    conv_bc_weight,
    step_bias,
    decay_log,
    skip_gain,
    group_gain,
    out_weight,
    scan_state,
    conv_x_state,
    conv_bc_state,
):
    n_tp, n_z = lax.axis_size(TP), lax.axis_size("z")
    plane = tuple(lax.axis_size(name) for name in CTP)
    rows_dev, cols_dev = stream.shape
    half = rows_dev // 2
    seq_count, heads_dev = scan_state.shape[1:3]
    x_width = x_weight.shape[2]
    bc_width = 2 * bc_weight.shape[3]
    seqs = n_z * seq_count
    in_blocks = (2 * x_width + bc_width) // LANES + 1
    out_blocks = x_width // LANES
    rest = in_blocks + LAYERS * out_blocks + 1
    wide = in_blocks * LANES
    shape = jax.ShapeDtypeStruct

    dma = pltpu.SemaphoreType.DMA
    bc_rows = bc_weight.reshape(LAYERS, 2 * cols_dev, LANES)
    small = (
        jnp.transpose(conv_x_weight, (1, 0, 2)), conv_bc_weight, step_bias, decay_log,
        skip_gain, group_gain, conv_x_state, conv_bc_state,
    )
    own, packed, packed_rest, params = pack(
        enter,
        (
            shape((2 * n_tp, half, cols_dev), bf16),
            shape((cols_dev, (in_blocks + 1) * LANES), bf16),
            shape((cols_dev, rest * LANES), bf16),
            shape((LAYERS, 8, x_width), f32),
        ),
        (pl.BlockSpec(memory_space=pl.ANY), VMEM, VMEM, VMEM),
        [
            pltpu.VMEM(stream.shape, bf16),
            pltpu.VMEM((2 * n_tp, half, cols_dev), bf16),
            pltpu.VMEM(bc_rows.shape, bf16),
            pltpu.VMEM(norm_gain.shape, f32),
            *(pltpu.VMEM(a.shape, a.dtype) for a in small),
            dma((in_blocks + 1,)),
            dma((rest,)),
            dma((len(small) + 4,)),
        ],
        stream, x_weight, z_weight, step_weight, out_weight, bc_rows, norm_gain, *small,
    )
    hidden = exchange_plane(own, CTP, plane)
    w_first = (packed, swap_cores(packed))
    w_rest = (packed_rest, swap_cores(packed_rest))

    result = None
    for l in range(LAYERS):
        if l == 0:
            hidden = hidden.reshape(2, seqs, cols_dev)
            part = call(
                functools.partial(project_first, in_blocks, heads_dev),
                shape((seqs, wide), bf16), 3, 10000000, 1000000,
            )(hidden, *w_first)
        else:
            part, hidden = call(
                functools.partial(project_next, in_blocks, heads_dev),
                (shape((seqs, wide), bf16), shape((2, seqs, cols_dev), bf16)), 4, 10000000, 1000000,
            )(arrived, hidden, *w_rest)
        got = exchange_z(part.reshape(n_z, seq_count, wide), n_z)
        mixed_shape = shape((n_z, seq_count, x_width), bf16)
        if l == 0:
            mixed, state_first, proj_first = call(
                functools.partial(scan_first, heads_dev),
                (
                    mixed_shape,
                    shape(scan_state.shape[1:], f32),
                    shape((seq_count, wide - LANES), bf16),
                ),
                3, 10000000, 1000000,
            )(got, params, scan_state)
        else:
            hbm = pl.BlockSpec(memory_space=pl.ANY)
            mixed, *outs = pl.pallas_call(
                functools.partial(scan_last, heads_dev),
                out_shape=(
                    mixed_shape,
                    shape(scan_state.shape, f32),
                    shape(conv_x_state.shape, bf16),
                    shape(conv_bc_state.shape, bf16),
                ),
                in_specs=[VMEM] * 7,
                out_specs=(VMEM, hbm, hbm, hbm),
                scratch_shapes=[
                    pltpu.VMEM(scan_state.shape[1:], f32),
                    pltpu.VMEM(conv_x_state.shape, bf16),
                    pltpu.VMEM(conv_bc_state.shape, bf16),
                    pltpu.SemaphoreType.DMA((seq_count + 3,)),
                ],
                name="scan_last",
                compiler_params=pltpu.CompilerParams(vmem_limit_bytes=8 * 1024 * 1024),
                cost_estimate=pl.CostEstimate(
                    flops=10000000, bytes_accessed=1000000, transcendentals=0
                ),
            )(got, params, scan_state, state_first, proj_first, conv_x_state, conv_bc_state)

        mixed = exchange_z(mixed, n_z).reshape(seqs, x_width)
        at = in_blocks + 1 + l * out_blocks
        if l + 1 < LAYERS:
            terms = call(
                functools.partial(mix_to_all, at, out_blocks),
                shape((n_tp, 2, seqs, cols_dev), bf16), 3, 10000000, 1000000,
            )(mixed, *w_rest)
            arrived = exchange_plane(terms, TP, plane[1:])
        else:
            terms = call(
                functools.partial(mix_last, at, out_blocks),
                shape((2, seqs, cols_dev), bf16), 3, 10000000, 1000000,
            )(mixed, *w_rest)
            both = jnp.concatenate(
                [terms.reshape(2 * n_tp, half, cols_dev), hidden.reshape(2 * n_tp, half, cols_dev)],
                axis=1,
            )
            got = exchange_plane(both, CTP, plane).reshape(2, n_tp, rows_dev, cols_dev).astype(f32)
            result = got[:, :, :half].sum(axis=1) + got[:, 0, half:]
            result = result[::-1].astype(bf16).reshape(rows_dev, cols_dev)
    return (result, *outs)


def solution(mesh):
    fine = Mesh(mesh.devices.reshape(4, 4, -1, 2), ("y", "x", "z", "core"))
    dp = ("z", "core")
    in_specs = (
        P(TP, dp),
        P(None, dp),
        P(None, dp, TP),
        P(None, dp, TP),
        P(None, dp, None, TP),
        P(None, dp, None),
        P(None, None, TP),
        P(None, None, None, TP),
        P(None, TP),
        P(None, TP),
        P(None, TP),
        P(None, TP),
        P(None, TP, dp),
        P(None, dp, TP, None, None),
        P(None, dp, None, TP),
        P(None, dp, None, None, TP),
    )
    out_specs = (
        P(TP, dp),
        P(None, dp, TP, None, None),
        P(None, dp, None, TP),
        P(None, dp, None, None, TP),
    )
    return jax.shard_map(shards, mesh=fine, in_specs=in_specs, out_specs=out_specs, check_vma=False)
```

```python
import functools

import jax
import jax.numpy as jnp
from jax import lax
from jax.experimental import pallas as pl
from jax.experimental.pallas import tpu as pltpu
from jax.sharding import Mesh, PartitionSpec as P


MODEL_WIDTH = 4096
HEAD_DIM = 64
STATE_DIM = 128
LAYERS = 2
EPS = 1e-06
LANES = 128

TP = ("y", "x")
CTP = ("core", "y", "x")
VMEM = pl.BlockSpec(memory_space=pltpu.VMEM)
f32, bf16 = jnp.float32, jnp.bfloat16


def from_middle(count):
    return [(count // 2 + k) % count for k in range(count)]


def exchange_z(value, count):
    return lax.all_to_all(
        value, "z", split_axis=0, concat_axis=0, axis_index_groups=[from_middle(count)], tiled=True
    )


def exchange_plane(value, axis, sizes):
    order = [0]
    for name, size in zip(axis, sizes):
        inner = from_middle(size)
        order = [at * size + k for at in order for k in inner]
    return lax.all_to_all(
        value, axis, split_axis=0, concat_axis=0, axis_index_groups=[order], tiled=True
    )


def swap_cores(value):
    return lax.ppermute(value, "core", [(0, 1), (1, 0)])


def call(body, out_shape, n_in, flops, size):
    return pl.pallas_call(
        body,
        out_shape=out_shape,
        in_specs=[VMEM] * n_in,
        out_specs=jax.tree.map(lambda _: VMEM, out_shape),
        compiler_params=pltpu.CompilerParams(vmem_limit_bytes=8 * 1024 * 1024),
        cost_estimate=pl.CostEstimate(flops=flops, bytes_accessed=size, transcendentals=0),
    )


def span(at, count=1):
    return pl.ds(at * LANES, count * LANES)


def projection_copies(layer, x_ref, z_ref, step_ref, out_ref, sems):
    copies = []
    at = 0
    for ref in (x_ref, z_ref, None, step_ref):
        if ref is None:
            at += 2
            continue
        count = ref.shape[2] // LANES
        target = out_ref.at[:, span(at, count)]
        copies.append(pltpu.make_async_copy(ref.at[layer], target, sems.at[at]))
        at += count
    return copies, at


def put_pair(both, out_ref, at):
    rows = both.shape[0]
    to = lax.broadcasted_iota(jnp.int32, (rows, rows), 0)
    source = lax.broadcasted_iota(jnp.int32, (rows, rows), 1)
    want = 2 * (to % (rows // 2)) + to // (rows // 2)
    pick = jnp.where(source == want, 1.0, 0.0).astype(bf16)
    parted = jnp.dot(pick, both, preferred_element_type=f32).astype(bf16)
    out_ref[:, span(at)] = parted[: rows // 2]
    out_ref[:, span(at + 1)] = parted[rows // 2 :]


def put_gain(gain, out_ref, at):
    first = gain.astype(bf16)
    left = gain - first.astype(f32)
    second = left.astype(bf16)
    third = (left - second.astype(f32)).astype(bf16)
    row = lax.broadcasted_iota(jnp.int32, (LANES, LANES), 0)
    pieces = jnp.where(row == 1, second.astype(f32), jnp.where(row == 2, third.astype(f32), 0.0))
    out_ref[:, span(at)] = jnp.where(row == 0, first.astype(f32), pieces).astype(bf16)


def enter(
    stream_ref, x_ref, z_ref, step_ref, w_ref, bc_ref, gain_ref,
    tap_x_ref, tap_bc_ref, bias_ref, decay_ref, skip_ref, group_ref, conv_x_ref, conv_bc_ref,
    own_out, out_ref, rest_ref, par_ref,
    stream_buf, own_buf, bc_buf, gain_buf,
    tap_x, tap_bc, bias, decay, skip, group, conv_x, conv_bc, sems, rest_sems, par_sems,
):
    into = pltpu.make_async_copy(stream_ref, stream_buf, par_sems.at[0])
    into.start()
    sources = (tap_x_ref, tap_bc_ref, bias_ref, decay_ref, skip_ref, group_ref)
    sources += (conv_x_ref, conv_bc_ref, bc_ref, gain_ref)
    bufs = (tap_x, tap_bc, bias, decay, skip, group, conv_x, conv_bc, bc_buf, gain_buf)
    loads = [
        pltpu.make_async_copy(a, b, par_sems.at[2 + k])
        for k, (a, b) in enumerate(zip(sources, bufs))
    ]
    for copy in loads[-2:]:
        copy.start()
    copies, gain_at = projection_copies(0, x_ref, z_ref, step_ref, out_ref, sems)
    others, _ = projection_copies(1, x_ref, z_ref, step_ref, rest_ref, rest_sems)
    at = gain_at + 1
    for l in range(LAYERS):
        for k in range(w_ref.shape[1] // LANES):
            block = w_ref.at[l, pl.ds(k * LANES, LANES), :]
            others.append(pltpu.make_async_copy(block, rest_ref.at[:, span(at)], rest_sems.at[at]))
            at += 1
    for copy in copies + loads[:-2] + others:
        copy.start()
    into.wait()
    half = own_buf.shape[1]
    each = own_buf.shape[0] // 2
    for c in range(2):
        rows = stream_buf[(1 - c) * half : (2 - c) * half]
        for p in range(each):
            own_buf[c * each + p] = rows
    out = pltpu.make_async_copy(own_buf, own_out, par_sems.at[1])
    out.start()
    for copy in loads:
        copy.wait()
    shared_at = 2 * (x_ref.shape[2] // LANES)
    for l, ref in ((0, out_ref), (1, rest_ref)):
        put_pair(bc_buf[l], ref, shared_at)
        put_gain(gain_buf[l : l + 1, :], ref, gain_at)
    heads = bias.shape[1]
    seqs = conv_x.shape[1]
    taps = tap_x.shape[0] - 1
    par_ref[...] = jnp.zeros(par_ref.shape, f32)
    for l in range(LAYERS):
        for s in range(seqs):
            old = conv_x[l, s].astype(f32)
            base = jnp.zeros((1, old.shape[1]), f32)
            pair = jnp.zeros((2, LANES), f32)
            for k in range(taps):
                base = base + old[k : k + 1] * tap_x[k].astype(f32)[l : l + 1]
                pair = pair + conv_bc[l, s, k].astype(f32) * tap_bc[l, k].astype(f32)
            par_ref[l, s : s + 1, :] = base
            par_ref[l, 4 + s : 5 + s, :LANES] = pair[0:1]
            par_ref[l, 4 + s : 5 + s, LANES : 2 * LANES] = pair[1:2]
        last = tap_bc[l, taps].astype(f32)
        par_ref[l, 2:3, :] = tap_x[taps].astype(f32)[l : l + 1]
        par_ref[l, 3:4, :] = group[l : l + 1, :]
        par_ref[l, 6:7, :LANES] = last[0:1]
        par_ref[l, 6:7, LANES : 2 * LANES] = last[1:2]
        par_ref[l, 7:8, :heads] = bias[l : l + 1, :]
        par_ref[l, 7:8, LANES : LANES + heads] = jnp.exp(decay[l : l + 1, :])
        par_ref[l, 7:8, 2 * LANES : 2 * LANES + heads] = skip[l : l + 1, :]
    for copy in copies + others + [out]:
        copy.wait()


def pack(body, out_shape, out_specs, scratch, *arrays):
    return pl.pallas_call(
        body,
        out_shape=out_shape,
        in_specs=[pl.BlockSpec(memory_space=pltpu.HBM)] * len(arrays),
        out_specs=out_specs,
        scratch_shapes=scratch,
        compiler_params=pltpu.CompilerParams(vmem_limit_bytes=8 * 1024 * 1024),
        cost_estimate=pl.CostEstimate(flops=1000000, bytes_accessed=1000000, transcendentals=0),
    )(*(pltpu.with_memory_space_constraint(a, pltpu.HBM) for a in arrays))


def swapped(rows):
    tiles = [pltpu.roll(rows[k : k + 8], 4, 0) for k in range(0, rows.shape[0], 8)]
    return jnp.concatenate(tiles, axis=0)


def project(normed, squares, first, weights, out_ref, blocks):
    total = None
    place = (lax.axis_index("y") * lax.axis_size("x") + lax.axis_index("x")) * first
    for rows, w_ref in zip(normed, weights):
        block = w_ref[:, : blocks * LANES]
        term = jnp.dot(rows, block, preferred_element_type=f32)
        total = term if total is None else total + term
    wide = (blocks - 1) * LANES
    lane = lax.broadcasted_iota(jnp.int32, (total.shape[0], LANES), 1)
    tail = pltpu.roll(total[:, wide:], LANES - place, 1)
    tail = jnp.where(lane == first, squares, tail)
    out_ref[:, :wide] = total[:, :wide].astype(bf16)
    out_ref[:, wide:] = tail.astype(bf16)


def scaled(rows, w_ref, blocks):
    pieces = w_ref[:8, span(blocks)].astype(f32)
    gain = pieces[0:1] + pieces[1:2] + pieces[2:3]
    return (rows * gain).astype(bf16)


def project_first(blocks, heads, hidden_ref, own_ref, other_ref, out_ref):
    core = 1 - lax.axis_index("core")
    rows = [hidden_ref[core], hidden_ref[1 - core]]
    wide = [swapped(r.astype(f32)) for r in rows]
    squares = jnp.sum(wide[0] * wide[0] + wide[1] * wide[1], axis=1, keepdims=True)
    weights = (own_ref, other_ref)
    normed = [scaled(r, w, blocks) for r, w in zip(wide, weights)]
    project(normed, squares, heads, weights, out_ref, blocks)


def project_next(
    blocks, heads, arrived_ref, hidden_ref, own_ref, other_ref, out_ref, next_ref
):
    core = 1 - lax.axis_index("core")
    rows = []
    weights = (own_ref, other_ref)
    for c in (core, 1 - core):
        summed = arrived_ref[0, c].astype(f32)
        for j in range(1, arrived_ref.shape[0]):
            summed = summed + arrived_ref[j, c].astype(f32)
        new = (hidden_ref[c].astype(f32) + summed).astype(bf16)
        next_ref[c] = new
        rows.append(new)
    wide = [swapped(r.astype(f32)) for r in rows]
    squares = jnp.sum(wide[0] * wide[0] + wide[1] * wide[1], axis=1, keepdims=True)
    normed = [scaled(r, w, blocks) for r, w in zip(wide, weights)]
    project(normed, squares, heads, weights, out_ref, blocks)


def out_terms(mixed_ref, w_ref, at, blocks):
    weights = jnp.concatenate([w_ref[:, span(at + k)] for k in range(blocks)], axis=0)
    return swapped(jnp.dot(mixed_ref[...], weights, preferred_element_type=f32)).astype(bf16)


def mix_to_all(at, blocks, mixed_ref, own_ref, other_ref, out_ref):
    core = 1 - lax.axis_index("core")
    for c, w_ref in ((core, own_ref), (1 - core, other_ref)):
        terms = out_terms(mixed_ref, w_ref, at, blocks)
        for j in range(out_ref.shape[0]):
            out_ref[j, c] = terms


def mix_last(at, blocks, mixed_ref, own_ref, other_ref, out_ref):
    core = 1 - lax.axis_index("core")
    for c, w_ref in ((core, own_ref), (1 - core, other_ref)):
        out_ref[c] = out_terms(mixed_ref, w_ref, at, blocks)


def leave(count, got_ref, out_ref):
    half = got_ref.shape[1] // 2
    sums = []
    for c in range(2):
        total = got_ref[c * count].astype(f32)
        for p in range(1, count):
            total = total + got_ref[c * count + p].astype(f32)
        sums.append(total[:half] + got_ref[c * count].astype(f32)[half:])
    out_ref[...] = jnp.concatenate([sums[1], sums[0]], axis=0).astype(bf16)


def head_spread(values, head_dim, count):
    lane = lax.broadcasted_iota(jnp.int32, (values.shape[0], LANES), 1)
    pieces = []
    for k in range(count // 2):
        low = jnp.broadcast_to(values[:, 2 * k : 2 * k + 1], lane.shape)
        high = jnp.broadcast_to(values[:, 2 * k + 1 : 2 * k + 2], lane.shape)
        pieces.append(jnp.where(lane < head_dim, low, high))
    return jnp.concatenate(pieces, axis=1)


def columns(rows):
    pad = jnp.zeros((8 - rows.shape[0], rows.shape[1]), f32)
    return jnp.transpose(jnp.concatenate([rows, pad], axis=0))


def silu(v):
    return v * jax.nn.sigmoid(v)


def projected(got_ref):
    total = got_ref[0].astype(f32)
    for z in range(1, got_ref.shape[0]):
        total = total + got_ref[z].astype(f32)
    return total


def scan(layer, total, heads, par_ref, state_ref, proj_done, state_done):
    width = par_ref.shape[2]
    seqs = total.shape[0]
    tail = total[:, total.shape[1] - LANES :]
    inv = lax.rsqrt(tail[:, heads : heads + 1] / MODEL_WIDTH + EPS)
    rounded = (total[:, : total.shape[1] - LANES] * inv).astype(bf16)
    proj = rounded.astype(f32)
    par = par_ref[layer]
    inputs_x = silu(par[0:2] + proj[:, :width] * par[2:3])
    bc_width = proj.shape[1] - 2 * width
    inputs_bc = silu(par[4:6, :bc_width] + proj[:, 2 * width :] * par[6:7, :bc_width])
    raw = tail * inv + par[7:8, :LANES]
    step = jnp.maximum(raw, 0.0) + jnp.log1p(jnp.exp(-jnp.abs(raw)))
    decay = jnp.exp(-step * par[7:8, LANES : 2 * LANES])
    u_rows = head_spread(step, HEAD_DIM, heads) * inputs_x
    u_cols = columns(u_rows)
    row = lax.broadcasted_iota(jnp.int32, (8, STATE_DIM), 0)
    b_rows, c_rows = inputs_bc[:, :STATE_DIM], inputs_bc[:, STATE_DIM:]
    reads = []
    for s in range(seqs):
        c_row = c_rows[s : s + 1]
        c_high = c_row.astype(bf16).astype(f32)
        c_both = jnp.where(row == 0, c_high, jnp.where(row == 1, c_row - c_high, 0.0))
        old = state_ref[layer, s].reshape(width, STATE_DIM)
        out = lax.dot_general(
            c_both.astype(bf16), old.astype(bf16), (((1,), (1,)), ((), ())),
            preferred_element_type=f32,
        )
        reads.append(out[0:1] + out[1:2])
    for s in range(seqs):
        new = []
        for h in range(heads):
            at = h * HEAD_DIM
            keep = jnp.broadcast_to(decay[s : s + 1, h : h + 1], (HEAD_DIM, STATE_DIM))
            add = u_cols[at : at + HEAD_DIM, s : s + 1] * b_rows[s : s + 1]
            new.append(state_ref[layer, s, h] * keep + add)
        state_done(s, new)
    proj_done(rounded)
    readout = head_spread(decay, HEAD_DIM, heads) * jnp.concatenate(reads, axis=0)
    readout = readout + u_rows * jnp.sum(b_rows * c_rows, axis=1, keepdims=True)
    readout = readout + head_spread(par[7:8, 2 * LANES : 3 * LANES], HEAD_DIM, heads) * inputs_x
    gated = readout * silu(proj[:, width : 2 * width])
    mean = jnp.sum(gated * gated, axis=1, keepdims=True) / width
    return (gated * lax.rsqrt(mean + EPS) * par[3:4]).astype(bf16)


def scan_first(heads, got_ref, par_ref, state_ref, mixed_ref, new_ref, proj_ref):
    def proj_done(proj):
        proj_ref[...] = proj

    def state_done(s, new):
        for h in range(heads):
            new_ref[s, h] = new[h]

    mixed = scan(0, projected(got_ref), heads, par_ref, state_ref, proj_done, state_done)
    for z in range(mixed_ref.shape[0]):
        mixed_ref[z] = mixed


def scan_last(
    heads, got_ref, par_ref, state_ref, first_ref, first_proj_ref, conv_x_ref, conv_bc_ref,
    mixed_ref, state_out, conv_x_out, conv_bc_out, new_buf, x_buf, bc_buf, sems,
):
    width = par_ref.shape[2]
    seqs = got_ref.shape[1]
    copies = [pltpu.make_async_copy(first_ref, state_out.at[0], sems.at[0])]
    copies[0].start()

    def proj_done(proj):
        x_row = lax.broadcasted_iota(jnp.int32, (4, width), 0)
        bc_row = lax.broadcasted_iota(jnp.int32, (2, STATE_DIM), 0)
        for l, source in ((0, first_proj_ref[...]), (1, proj)):
            source = source.astype(f32)
            for s in range(seqs):
                old = conv_x_ref[l, s].astype(f32)
                rows = jnp.where(x_row == 2, old[3:4], source[s : s + 1, :width])
                rows = jnp.where(x_row == 1, old[2:3], rows)
                rows = jnp.where(x_row == 0, old[1:2], rows)
                x_buf[l, s] = rows.astype(bf16)
                for k in range(3):
                    bc_buf[l, s, k] = conv_bc_ref[l, s, k + 1]
                b_row = source[s : s + 1, 2 * width : 2 * width + STATE_DIM]
                c_row = source[s : s + 1, 2 * width + STATE_DIM :]
                bc_buf[l, s, 3] = jnp.where(bc_row == 0, b_row, c_row).astype(bf16)

    def state_done(s, new):
        for h in range(heads):
            new_buf[s, h] = new[h]
        copies.append(pltpu.make_async_copy(new_buf.at[s], state_out.at[1, s], sems.at[1 + s]))
        copies[-1].start()

    mixed = scan(1, projected(got_ref), heads, par_ref, state_ref, proj_done, state_done)
    for buf, out in ((x_buf, conv_x_out), (bc_buf, conv_bc_out)):
        copies.append(pltpu.make_async_copy(buf, out, sems.at[len(copies)]))
        copies[-1].start()
    for z in range(mixed_ref.shape[0]):
        mixed_ref[z] = mixed
    for copy in copies:
        copy.wait()


def shards(
    stream,
    norm_gain,
    x_weight,
    z_weight,
    bc_weight,
    step_weight,
    conv_x_weight,
    conv_bc_weight,
    step_bias,
    decay_log,
    skip_gain,
    group_gain,
    out_weight,
    scan_state,
    conv_x_state,
    conv_bc_state,
):
    n_tp, n_z = lax.axis_size(TP), lax.axis_size("z")
    plane = tuple(lax.axis_size(name) for name in CTP)
    rows_dev, cols_dev = stream.shape
    half = rows_dev // 2
    seq_count, heads_dev = scan_state.shape[1:3]
    x_width = x_weight.shape[2]
    bc_width = 2 * bc_weight.shape[3]
    seqs = n_z * seq_count
    in_blocks = (2 * x_width + bc_width) // LANES + 1
    out_blocks = x_width // LANES
    rest = in_blocks + LAYERS * out_blocks + 1
    wide = in_blocks * LANES
    shape = jax.ShapeDtypeStruct

    dma = pltpu.SemaphoreType.DMA
    bc_rows = bc_weight.reshape(LAYERS, 2 * cols_dev, LANES)
    small = (
        jnp.transpose(conv_x_weight, (1, 0, 2)), conv_bc_weight, step_bias, decay_log,
        skip_gain, group_gain, conv_x_state, conv_bc_state,
    )
    own, packed, packed_rest, params = pack(
        enter,
        (
            shape((2 * n_tp, half, cols_dev), bf16),
            shape((cols_dev, (in_blocks + 1) * LANES), bf16),
            shape((cols_dev, rest * LANES), bf16),
            shape((LAYERS, 8, x_width), f32),
        ),
        (pl.BlockSpec(memory_space=pl.ANY), VMEM, VMEM, VMEM),
        [
            pltpu.VMEM(stream.shape, bf16),
            pltpu.VMEM((2 * n_tp, half, cols_dev), bf16),
            pltpu.VMEM(bc_rows.shape, bf16),
            pltpu.VMEM(norm_gain.shape, f32),
            *(pltpu.VMEM(a.shape, a.dtype) for a in small),
            dma((in_blocks + 1,)),
            dma((rest,)),
            dma((len(small) + 4,)),
        ],
        stream, x_weight, z_weight, step_weight, out_weight, bc_rows, norm_gain, *small,
    )
    hidden = exchange_plane(own, CTP, plane)
    w_first = (packed, swap_cores(packed))
    w_rest = (packed_rest, swap_cores(packed_rest))

    result = None
    for l in range(LAYERS):
        if l == 0:
            hidden = hidden.reshape(2, seqs, cols_dev)
            part = call(
                functools.partial(project_first, in_blocks, heads_dev),
                shape((seqs, wide), bf16), 3, 10000000, 1000000,
            )(hidden, *w_first)
        else:
            part, hidden = call(
                functools.partial(project_next, in_blocks, heads_dev),
                (shape((seqs, wide), bf16), shape((2, seqs, cols_dev), bf16)), 4, 10000000, 1000000,
            )(arrived, hidden, *w_rest)
        got = exchange_z(part.reshape(n_z, seq_count, wide), n_z)
        mixed_shape = shape((n_z, seq_count, x_width), bf16)
        if l == 0:
            mixed, state_first, proj_first = call(
                functools.partial(scan_first, heads_dev),
                (
                    mixed_shape,
                    shape(scan_state.shape[1:], f32),
                    shape((seq_count, wide - LANES), bf16),
                ),
                3, 10000000, 1000000,
            )(got, params, scan_state)
        else:
            hbm = pl.BlockSpec(memory_space=pl.ANY)
            mixed, *outs = pl.pallas_call(
                functools.partial(scan_last, heads_dev),
                out_shape=(
                    mixed_shape,
                    shape(scan_state.shape, f32),
                    shape(conv_x_state.shape, bf16),
                    shape(conv_bc_state.shape, bf16),
                ),
                in_specs=[VMEM] * 7,
                out_specs=(VMEM, hbm, hbm, hbm),
                scratch_shapes=[
                    pltpu.VMEM(scan_state.shape[1:], f32),
                    pltpu.VMEM(conv_x_state.shape, bf16),
                    pltpu.VMEM(conv_bc_state.shape, bf16),
                    pltpu.SemaphoreType.DMA((seq_count + 3,)),
                ],
                name="scan_last",
                compiler_params=pltpu.CompilerParams(vmem_limit_bytes=8 * 1024 * 1024),
                cost_estimate=pl.CostEstimate(
                    flops=10000000, bytes_accessed=1000000, transcendentals=0
                ),
            )(got, params, scan_state, state_first, proj_first, conv_x_state, conv_bc_state)

        mixed = exchange_z(mixed, n_z).reshape(seqs, x_width)
        at = in_blocks + 1 + l * out_blocks
        if l + 1 < LAYERS:
            terms = call(
                functools.partial(mix_to_all, at, out_blocks),
                shape((n_tp, 2, seqs, cols_dev), bf16), 3, 10000000, 1000000,
            )(mixed, *w_rest)
            arrived = exchange_plane(terms, TP, plane[1:])
        else:
            terms = call(
                functools.partial(mix_last, at, out_blocks),
                shape((2, seqs, cols_dev), bf16), 3, 10000000, 1000000,
            )(mixed, *w_rest)
            both = jnp.concatenate(
                [terms.reshape(2 * n_tp, half, cols_dev), hidden.reshape(2 * n_tp, half, cols_dev)],
                axis=1,
            )
            got = exchange_plane(both, CTP, plane)
            result = call(
                functools.partial(leave, n_tp), shape((rows_dev, cols_dev), bf16),
                1, 100000, 100000,
            )(got)
    return (result, *outs)


def solution(mesh):
    fine = Mesh(mesh.devices.reshape(4, 4, -1, 2), ("y", "x", "z", "core"))
    dp = ("z", "core")
    in_specs = (
        P(TP, dp),
        P(None, dp),
        P(None, dp, TP),
        P(None, dp, TP),
        P(None, dp, None, TP),
        P(None, dp, None),
        P(None, None, TP),
        P(None, None, None, TP),
        P(None, TP),
        P(None, TP),
        P(None, TP),
        P(None, TP),
        P(None, TP, dp),
        P(None, dp, TP, None, None),
        P(None, dp, None, TP),
        P(None, dp, None, None, TP),
    )
    out_specs = (
        P(TP, dp),
        P(None, dp, TP, None, None),
        P(None, dp, None, TP),
        P(None, dp, None, None, TP),
    )
    return jax.shard_map(shards, mesh=fine, in_specs=in_specs, out_specs=out_specs, check_vma=False)
```
